32 devices in a mesh: sp: 8 (over z, y), tp: 4 (over x, core).
Axes of the slice: x: 2, y: 2, z: 4, core: 2. Of those that a mesh axis runs over, the one named last changes fastest.
Arguments:
- queries: bfloat16 [4096, 2048], P('sp', 'tp'), may hold values from -8 to 8
- keys: bfloat16 [4096, 512], P('sp', 'tp'), may hold values from -8 to 8
- values: bfloat16 [4096, 512], P('sp', 'tp'), may hold values from -6 to 6
- q_gain: float32 [128], replicated, may hold values from 0.1 to 5.8
- k_gain: float32 [128], replicated, may hold values from 0.1 to 5.8
- out_weight: bfloat16 [2048, 2048], replicated, may hold values from -0.125 to 0.125
- out_gain: float32 [2048], replicated, may hold values from 0.1 to 1.9
- residual_in: bfloat16 [4096, 2048], P(('sp', 'tp')), may hold values from -6 to 6
- mlp_gain: float32 [2048], replicated, may hold values from 0.1 to 1.9
- gate_weight: bfloat16 [2048, 5632], P('sp', 'tp'), may hold values from -0.125 to 0.125
- up_weight: bfloat16 [2048, 5632], P('sp', 'tp'), may hold values from -0.125 to 0.125
- down_weight: bfloat16 [5632, 2048], P('tp', 'sp'), may hold values from -0.078125 to 0.078125
- final_gain: float32 [2048], replicated, may hold values from 0.1 to 1.9
Outputs:
- layer_out: bfloat16 [4096, 2048], P(('sp', 'tp'))
The draws below stay inside these ranges and needn't reach their ends.
All inputs are finite; a program needn't handle non-finite values.
Results may differ from the reference program's by a relative error of at most 0.015.
The reference program's roundings to bfloat16 on the way count: a program that leaves them out, or rounds other values in their place, can miss the bound.
Values may be sent and summed in bfloat16 or wider, within the bound.
A program may use at most 128 MiB of HBM per device.

```python
import jax
import jax.numpy as jnp
from jax import lax

D = 2048
HQ = 16
KV = 4
HD = 128
FF = 5632
GRID_W = 64
TOK_DEV = 512
TOKENS = 4096


def drawn(base_key):
    query_base = jnp.clip(jax.random.normal(jax.random.fold_in(base_key, 101), (TOKENS, HQ, HD), jnp.float32), -6.0, 6.0)
    key_base = jnp.clip(jax.random.normal(jax.random.fold_in(base_key, 102), (TOKENS, KV, HD), jnp.float32), -6.0, 6.0)
    return (query_base.reshape(TOKENS, HQ * HD), key_base.reshape(TOKENS, KV * HD))


def gain_values(base_key):
    return 1.0 + 0.18 * jnp.clip(jax.random.normal(base_key, (HD,), jnp.float32), -5.0, 5.0)


def draw_queries(key, part):
    return drawn(key)[0].astype(jnp.bfloat16)


def draw_keys(key, part):
    return drawn(key)[1].astype(jnp.bfloat16)


def draw_q_gain(key, part):
    return gain_values(jax.random.fold_in(key, 201))


def draw_k_gain(key, part):
    return gain_values(jax.random.fold_in(key, 202))


def level_of(own_key, shape, shards, smallest, largest):
    gain, own = 1.0, jax.random.fold_in(own_key, 6)
    for position, shards_of in shards:
        draws = jnp.exp(jax.random.uniform(jax.random.fold_in(own, position), (shards_of,), jnp.float32, smallest / len(shards), largest / len(shards)))
        gain = gain * jnp.repeat(draws, shape[position] // shards_of).reshape([-1 if axis == position else 1 for axis in range(len(shape))])
    return gain


def scatter_about(key, extent, spread, bound, shards=(), kind=jnp.bfloat16):
    loudness = level_of(key, extent, shards, -0.22, 0.18) if shards else 1.0
    entries = jax.random.normal(key, extent, jnp.float32) * spread * loudness
    return jnp.minimum(jnp.maximum(entries, -bound), bound).astype(kind)


def setup_inputs(seed: int = 0) -> dict:
    splits = jax.random.split(jax.random.key(seed), 14)
    queries = draw_queries(jax.random.fold_in(splits[13], 71), 0)
    keys = draw_keys(jax.random.fold_in(splits[13], 71), 0)
    values = scatter_about(splits[2], (TOKENS, KV * HD), 1.0, 6.0, ((0, 8), (1, 4)))
    q_gain = draw_q_gain(jax.random.fold_in(splits[13], 71), 0)
    k_gain = draw_k_gain(jax.random.fold_in(splits[13], 71), 0)
    out_weight = scatter_about(splits[5], (HQ * HD, D), (HQ * HD) ** -0.5, 0.125)
    out_gain = jnp.clip(1.0 + 0.18 * jax.random.normal(splits[6], (D,), jnp.float32), 0.1, 1.9)
    residual_in = scatter_about(splits[7], (TOKENS, D), 1.0, 6.0, ((0, 32),))
    mlp_gain = jnp.clip(1.0 + 0.18 * jax.random.normal(splits[8], (D,), jnp.float32), 0.1, 1.9)
    gate_weight = scatter_about(splits[9], (D, FF), D ** -0.5, 0.125, ((0, 8), (1, 4)))
    up_weight = scatter_about(splits[10], (D, FF), D ** -0.5, 0.125, ((0, 8), (1, 4)))
    down_weight = scatter_about(splits[11], (FF, D), FF ** -0.5, 0.078125, ((0, 4), (1, 8)))
    final_gain = jnp.clip(1.0 + 0.18 * jax.random.normal(splits[12], (D,), jnp.float32), 0.1, 1.9)
    return dict(queries=queries, keys=keys, values=values, q_gain=q_gain, k_gain=k_gain, out_weight=out_weight, out_gain=out_gain, residual_in=residual_in, mlp_gain=mlp_gain, gate_weight=gate_weight, up_weight=up_weight, down_weight=down_weight, final_gain=final_gain)


def rms_scale(matrix):
    return matrix * lax.rsqrt(lax.optimization_barrier(jnp.mean(matrix * matrix, axis=-1, keepdims=True)) + 1e-06)

def rotary(matrix, positions):
    quarter = matrix.shape[-1] // 4
    freqs = 10000.0 ** (-jnp.arange(quarter, dtype=jnp.float32) / quarter)
    grid = jnp.stack([positions // GRID_W, positions % GRID_W], axis=-1).astype(jnp.float32)
    angle = grid[:, :, None] * freqs
    cosine = jnp.cos(angle)[:, None]
    sine = jnp.sin(angle)[:, None]
    parts = matrix.reshape(matrix.shape[:-1] + (2, 2, quarter))
    first = parts[..., 0, :]
    second = parts[..., 1, :]
    turned = jnp.stack([first * cosine - second * sine, second * cosine + first * sine], axis=-2)
    return turned.reshape(matrix.shape)

def reference(queries, keys, values, q_gain, k_gain, out_weight, out_gain, residual_in, mlp_gain, gate_weight, up_weight, down_weight, final_gain):
    tok_total = queries.shape[0]
    positions = jnp.arange(tok_total, dtype=jnp.int32)
    query_rot = rotary(rms_scale(queries.reshape(tok_total, HQ, HD).astype(jnp.float32)) * q_gain, positions).astype(jnp.bfloat16)
    key_rot = rotary(rms_scale(keys.reshape(tok_total, KV, HD).astype(jnp.float32)) * k_gain, positions).astype(jnp.bfloat16)
    value_heads = values.reshape(tok_total, KV, HD)
    group_size = HQ // KV
    score_scale = HD ** (-0.5)

    def one_head(head_index):
        query_head = lax.dynamic_index_in_dim(query_rot, head_index, 1, keepdims=False)
        key_head = lax.dynamic_index_in_dim(key_rot, head_index // group_size, 1, keepdims=False)
        value_head = lax.dynamic_index_in_dim(value_heads, head_index // group_size, 1, keepdims=False)

        def one_block(query_block):
            scores = jnp.dot(query_block, key_head.T, preferred_element_type=jnp.float32) * score_scale
            highest = lax.optimization_barrier(jnp.max(scores, axis=-1, keepdims=True))
            exp_scores = jnp.exp(scores - highest)
            weight_sum = lax.optimization_barrier(jnp.sum(exp_scores, axis=-1, keepdims=True))
            mixed = jnp.dot(exp_scores.astype(jnp.bfloat16), value_head, preferred_element_type=jnp.float32) / weight_sum
            return mixed.astype(jnp.bfloat16)
        blocks = query_head.reshape(tok_total // TOK_DEV, TOK_DEV, HD)
        return lax.map(one_block, blocks).reshape(tok_total, HD)
    per_head = lax.map(one_head, jnp.arange(HQ, dtype=jnp.int32))
    attended = jnp.transpose(per_head, (1, 0, 2)).reshape(tok_total, HQ * HD)
    projected = jnp.dot(attended, out_weight, preferred_element_type=jnp.float32)
    mid_stream = (residual_in.astype(jnp.float32) + out_gain * rms_scale(projected)).astype(jnp.bfloat16)
    normed = (mlp_gain * rms_scale(mid_stream.astype(jnp.float32))).astype(jnp.bfloat16)
    gate_proj = jnp.dot(normed, gate_weight, preferred_element_type=jnp.float32)
    up_proj = jnp.dot(normed, up_weight, preferred_element_type=jnp.float32)
    hidden = (jax.nn.silu(gate_proj) * up_proj).astype(jnp.bfloat16)
    mlp_branch = jnp.dot(hidden, down_weight, preferred_element_type=jnp.float32)
    return (mid_stream.astype(jnp.float32) + final_gain * rms_scale(mlp_branch)).astype(jnp.bfloat16)
```

```python
import functools
import math

import jax
import jax.numpy as jnp
from jax import lax
from jax.experimental import pallas as pl
from jax.experimental.pallas import tpu as pltpu
from jax.sharding import PartitionSpec as P

GRID_W = 64


def rms_scale(matrix):
    return matrix * lax.rsqrt(jnp.mean(matrix * matrix, axis=-1, keepdims=True) + 1e-06)


def rotary(matrix, positions):
    quarter = matrix.shape[-1] // 4
    freqs = 10000.0 ** (-jnp.arange(quarter, dtype=jnp.float32) / quarter)
    grid = jnp.stack([positions // GRID_W, positions % GRID_W], axis=-1).astype(jnp.float32)
    angle = grid[:, :, None] * freqs
    cosine = jnp.cos(angle)[:, None]
    sine = jnp.sin(angle)[:, None]
    parts = matrix.reshape(matrix.shape[:-1] + (2, 2, quarter))
    first = parts[..., 0, :]
    second = parts[..., 1, :]
    turned = jnp.stack([first * cosine - second * sine, second * cosine + first * sine], axis=-2)
    return turned.reshape(matrix.shape)


def on_device(
    queries,
    keys,
    values,
    q_gain,
    k_gain,
    out_weight,
    out_gain,
    residual_in,
    mlp_gain,
    gate_weight,
    up_weight,
    down_weight,
    final_gain,
):
    tok_rows = queries.shape[0]
    head_size = q_gain.shape[0]
    q_heads = queries.shape[1] // head_size
    kv_heads = keys.shape[1] // head_size
    group_size = q_heads // kv_heads
    positions = lax.axis_index("sp") * tok_rows + jnp.arange(tok_rows, dtype=jnp.int32)
    query_rot = rotary(
        rms_scale(queries.reshape(tok_rows, q_heads, head_size).astype(jnp.float32)) * q_gain,
        positions,
    ).astype(jnp.bfloat16)
    key_rot = rotary(
        rms_scale(keys.reshape(tok_rows, kv_heads, head_size).astype(jnp.float32)) * k_gain,
        positions,
    ).astype(jnp.bfloat16)
    key_flat = key_rot.reshape(tok_rows, kv_heads * head_size)
    grouped = query_rot.reshape(tok_rows, kv_heads, group_size, head_size)
    score_scale = head_size ** (-0.5)
    key_all, value_all = (
        lax.all_gather(key_flat, "sp", axis=0, tiled=True),
        lax.all_gather(values, "sp", axis=0, tiled=True),
    )
    total_rows = key_all.shape[0]
    span = math.gcd(total_rows, 1024)
    key_blocks = key_all.reshape(total_rows // span, span, kv_heads, head_size)
    value_blocks = value_all.reshape(total_rows // span, span, kv_heads, head_size)

    def step(run_state, blocks):
        highest, weight_sum, accum = run_state
        key_block, value_block = blocks
        scores = (
            jnp.einsum("qcgd,kcd->cgqk", grouped, key_block, preferred_element_type=jnp.float32)
            * score_scale
        )
        new_high = jnp.maximum(highest, jnp.max(scores, axis=-1))
        factor = jnp.exp(highest - new_high)
        exp_scores = jnp.exp(scores - new_high[..., None])
        weight_sum = weight_sum * factor + jnp.sum(exp_scores, axis=-1)
        accum = accum * factor[..., None] + jnp.einsum(
            "cgqk,kcd->cgqd",
            exp_scores.astype(jnp.bfloat16),
            value_block,
            preferred_element_type=jnp.float32,
        )
        return ((new_high, weight_sum, accum), None)

    start_state = (
        jnp.full((kv_heads, group_size, tok_rows), -1e30, jnp.float32),
        jnp.zeros((kv_heads, group_size, tok_rows), jnp.float32),
        jnp.zeros((kv_heads, group_size, tok_rows, head_size), jnp.float32),
    )
    final_state, unused = lax.scan(step, start_state, (key_blocks, value_blocks))
    highest, weight_sum, accum = final_state
    attended = (
        jnp.transpose(accum / weight_sum[..., None], (2, 0, 1, 3))
        .reshape(tok_rows, q_heads * head_size)
        .astype(jnp.bfloat16)
    )
    head_rows = lax.all_to_all(attended, "tp", split_axis=0, concat_axis=1, tiled=True)
    projected = jnp.dot(head_rows, out_weight, preferred_element_type=jnp.float32)
    mid_stream = (residual_in.astype(jnp.float32) + out_gain * rms_scale(projected)).astype(
        jnp.bfloat16
    )
    normed = (mlp_gain * rms_scale(mid_stream.astype(jnp.float32))).astype(jnp.bfloat16)
    mixer_in = lax.all_gather(normed, "tp", axis=0, tiled=True)
    gate_proj = jnp.dot(
        mixer_in,
        lax.all_gather(gate_weight, "sp", axis=0, tiled=True),
        preferred_element_type=jnp.float32,
    )
    up_proj = jnp.dot(
        mixer_in,
        lax.all_gather(up_weight, "sp", axis=0, tiled=True),
        preferred_element_type=jnp.float32,
    )
    down_full = lax.all_gather(down_weight, "sp", axis=1, tiled=True)
    hidden = (jax.nn.silu(gate_proj) * up_proj).astype(jnp.bfloat16)
    mlp_branch = lax.psum_scatter(
        jnp.dot(hidden, down_full, preferred_element_type=jnp.float32).astype(jnp.bfloat16),
        "tp",
        scatter_dimension=0,
        tiled=True,
    ).astype(jnp.float32)
    return (mid_stream.astype(jnp.float32) + final_gain * rms_scale(mlp_branch)).astype(
        jnp.bfloat16
    )


MESH = pl.DeviceIdType.MESH
EPS = 1e-06


def layer_kernel(
    n,
    tn,
    q_in,
    k_in,
    v_hbm,
    cos_ref,
    sin_ref,
    qg_ref,
    kg_ref,
    ow_hbm,
    og_ref,
    res_ref,
    mg_ref,
    gate_hbm,
    up_hbm,
    down_hbm,
    fg_ref,
    out_ref,
    qs,
    kbuf,
    vbuf,
    vraw,
    raw,
    wt,
    wall,
    ow,
    m_s,
    l_s,
    acc,
    att,
    heads,
    proj,
    mid,
    toks,
    inner,
    osc,
    psend,
    precv,
    loc_sem,
    send_sem,
    recv_sem,
    tp_send,
    tp_recv,
    w_send,
    w_recv,
    t_send,
    t_recv,
    p_send,
    p_recv,
):
    sp = lax.axis_index("sp")
    tp = lax.axis_index("tp")
    half = n // 2
    nz = n // 2

    def ring_at(pos):
        pos = lax.rem(pos + 2 * n, n)
        return jnp.where(pos < half, 2 * pos, 2 * (n - 1 - pos) + 1)

    z, y = sp // 2, lax.rem(sp, 2)
    pos = jnp.where(y == 0, z, n - 1 - z)
    right, left = ring_at(pos + 1), ring_at(pos - 1)
    other_y = 1 - y
    y_dev = (sp + 1 - 2 * y, tp)
    x_dev = (sp, lax.rem(tp + tn // 2, tn))
    c_dev = (sp, tp + 1 - 2 * lax.rem(tp, 2))
    tok, hd = k_in.shape
    groups = q_in.shape[1] // hd
    depth = gate_hbm.shape[0]
    hidden = gate_hbm.shape[1]
    rows, wide = res_ref.shape
    width = groups * hd
    hq = hidden // nz
    units = hq * tn

    locs = {
        "v": pltpu.make_async_copy(v_hbm, vraw, loc_sem.at[0]),
        "g": pltpu.make_async_copy(gate_hbm, raw.at[0], loc_sem.at[1]),
        "u": pltpu.make_async_copy(up_hbm, raw.at[1], loc_sem.at[2]),
        "d": pltpu.make_async_copy(down_hbm, wt.at[2], loc_sem.at[3]),
        "o": pltpu.make_async_copy(ow_hbm, ow, loc_sem.at[4]),
    }
    for name in "vgudo":
        locs[name].start()

    lane = lax.broadcasted_iota(jnp.int32, (tok, hd), 1)
    quarter = hd // 4
    first = lax.rem(lane, 2 * quarter) < quarter

    def turned(x, gain):
        x = x.astype(jnp.float32)
        x = x * lax.rsqrt(jnp.mean(x * x, axis=-1, keepdims=True) + EPS) * gain
        other = jnp.where(first, pltpu.roll(x, hd - quarter, 1), pltpu.roll(x, quarter, 1))
        return (x * cos_ref[...] + other * sin_ref[...]).astype(jnp.bfloat16)

    kbuf[sp] = turned(k_in[...], kg_ref[...])

    barrier = pltpu.get_barrier_semaphore()
    for d in range(1, n):
        pl.semaphore_signal(
            barrier, inc=1, device_id=(lax.rem(sp + d, n), tp), device_id_type=MESH
        )
    for d in range(1, tn):
        pl.semaphore_signal(
            barrier, inc=1, device_id=(sp, lax.rem(tp + d, tn)), device_id_type=MESH
        )
    pl.semaphore_wait(barrier, n - 1 + tn - 1)

    started = []

    def start(copy):
        copy.start()
        started.append(copy)

    items = {
        "k": (0, half, lambda s: kbuf.at[s]),
        "v": (1, half - 1, lambda s: vbuf.at[s]),
    }

    def ring_copy(name, way, step, origin):
        number, to_right, view = items[name]
        index = (number * 2 + way) * half + step - 1
        return pltpu.make_async_remote_copy(
            src_ref=view(origin),
            dst_ref=view(origin),
            send_sem=send_sem.at[index],
            recv_sem=recv_sem.at[index],
            device_id=(right if way == 0 else left, tp),
            device_id_type=MESH,
        )

    def counts(name):
        to_right = items[name][1]
        return ((0, to_right), (1, n - 1 - to_right))

    def send(name):
        for way, count in counts(name):
            start(ring_copy(name, way, 1, sp))

    def arrive(name, step):
        for way, count in counts(name):
            if step > count:
                continue
            origin = ring_at(pos - step) if way == 0 else ring_at(pos + step)
            ring_copy(name, way, step, origin).wait_recv()
            if step < count:
                start(ring_copy(name, way, step + 1, origin))

    bases = {"z": 0, "x": 1, "y": 2, "d": 3, "cz": 4, "cy": 5, "cx": 6, "cd": 7}
    grain = {k: [(0, 3)] for k in range(nz)}
    grain[nz - 1] = [(0, 1), (1, 1), (2, 1)]

    def column(k, side):
        return 2 * lax.rem(z + k, nz) + side

    def piece(slot, r, part):
        return wall.at[slot, part[0] : part[0] + part[1], r * hq : (r + 1) * hq, :]

    def weight_copy(kind, k, part):
        index = (bases[kind] * nz + k) * 3 + part[0]
        if kind == "x":
            slot, r_from, r_to, dev = column(k, y), 0, 2, x_dev
        elif kind == "y":
            slot, r_from, r_to, dev = column(k, y), 0, 0, y_dev
        elif kind == "d" and k % 2 == 0:
            slot, r_from, r_to, dev = column(k, other_y), 0, 2, x_dev
        elif kind == "d":
            slot, r_from, r_to, dev = column(k, y), 2, 2, y_dev
        else:
            r_from = 0 if kind in ("cz", "cy") else 2
            r_to, dev = r_from + 1, c_dev
            slot = column(k, y if kind in ("cz", "cx") else other_y)
        return pltpu.make_async_remote_copy(
            src_ref=piece(slot, r_from, part),
            dst_ref=piece(slot, r_to, part),
            send_sem=w_send.at[index],
            recv_sem=w_recv.at[index],
            device_id=dev,
            device_id_type=MESH,
        )

    def weight_wait(kind, k, part):
        index = (bases[kind] * nz + k) * 3 + part[0]
        side = y if kind in ("z", "x", "cz", "cx") else other_y
        r = {"z": 0, "y": 0, "x": 2, "d": 2, "cz": 1, "cy": 1, "cx": 3, "cd": 3}[kind]
        here = piece(column(k, side), r, part)
        pltpu.make_async_remote_copy(
            src_ref=here,
            dst_ref=here,
            send_sem=w_send.at[index],
            recv_sem=w_recv.at[index],
            device_id=c_dev,
            device_id_type=MESH,
        ).wait_recv()

    spread_list = [(k, which) for k in range(1, nz) for which in range(3)]

    def spread(count):
        for k, which in spread_list[:count]:
            target = lax.rem(z - k + nz, nz)
            index = (bases["z"] * nz + k) * 3 + which
            start(
                pltpu.make_async_remote_copy(
                    src_ref=wt.at[
                        which : which + 1, pl.ds(pl.multiple_of(target * hq, 16), hq), :
                    ],
                    dst_ref=wall.at[sp, which : which + 1, 0:hq, :],
                    send_sem=w_send.at[index],
                    recv_sem=w_recv.at[index],
                    device_id=(2 * target + y, tp),
                    device_id_type=MESH,
                )
            )
        del spread_list[:count]

    def hop_own(k):
        for part in grain[k]:
            if k > 0:
                for which in range(part[0], part[0] + part[1]):
                    weight_wait("z", k, (which, 1))
            for kind in ("y", "x", "cz"):
                start(weight_copy(kind, k, part))

    def hop_side(k):
        for part in grain[k]:
            weight_wait("y", k, part)
            if k % 2 == 0:
                start(weight_copy("d", k, part))
            start(weight_copy("cy", k, part))
            weight_wait("x", k, part)
            if k % 2 == 1:
                start(weight_copy("d", k, part))
            start(weight_copy("cx", k, part))

    def hop_far(k):
        for part in grain[k]:
            weight_wait("d", k, part)
            start(weight_copy("cd", k, part))

    send("k")
    locs["v"].wait()
    vbuf[sp] = vraw[...].T
    send("v")
    locs["g"].wait()
    locs["u"].wait()

    def transpose(i, carry):
        part = pl.ds(pl.multiple_of(i * 128, 128), 128)
        for which in range(2):
            wt[which, part, :] = raw[which, :, part].T
        return carry

    lax.fori_loop(0, hidden // 128, transpose, 0)
    locs["d"].wait()
    own_piece = pltpu.make_async_copy(
        wt.at[:, pl.ds(pl.multiple_of(z * hq, 16), hq), :], wall.at[sp, :, 0:hq, :], loc_sem.at[5]
    )
    own_piece.start()
    spread(1)
    own_piece.wait()
    hop_own(0)

    for h in range(groups):
        qs[h] = turned(q_in[:, h * hd : (h + 1) * hd], qg_ref[...]).T
    m_s[...] = jnp.full_like(m_s, -1e30)
    l_s[...] = jnp.zeros_like(l_s)
    acc[...] = jnp.zeros_like(acc)
    factor = hd ** (-0.5) * math.log2(math.e)

    def attend(slots):
        def one(i, carry):
            h = lax.rem(i, groups)
            slot = slots[0]
            if len(slots) > 1:
                slot = jnp.where(i < groups, slots[0], slots[1])
            scores = jnp.dot(kbuf[slot], qs[h], preferred_element_type=jnp.float32)
            before = m_s[h]
            highest = jnp.maximum(before, jnp.max(scores, axis=0, keepdims=True))
            scale = jnp.exp2((before - highest) * factor)
            probs = jnp.exp2((scores - highest) * factor)
            m_s[h] = highest
            l_s[h] = l_s[h] * scale + jnp.sum(probs, axis=0, keepdims=True)
            acc[h] = acc[h] * scale + jnp.dot(
                vbuf[slot], probs.astype(jnp.bfloat16), preferred_element_type=jnp.float32
            )
            return carry

        lax.fori_loop(0, groups * len(slots), one, 0)

    attend([sp])
    for step in range(1, half + 1):
        arrive("k", step)
        arrive("v", step)
        spread(1 if step < half - 1 else len(spread_list))
        if step == half - 1:
            hop_side(0)
        ends = [ring_at(pos - step), ring_at(pos + step)]
        attend(ends if step < half else ends[:1])

    for h in range(groups):
        done = (acc[h] / l_s[h]).astype(jnp.bfloat16)
        for t in range(tn):
            att[t, :, h * hd : (h + 1) * hd] = done[:, t * rows : (t + 1) * rows].T
    to_heads = []
    for d in range(1, tn):
        peer = lax.rem(tp + d, tn)
        copy = pltpu.make_async_remote_copy(
            src_ref=att.at[peer],
            dst_ref=heads.at[tp],
            send_sem=tp_send.at[d - 1],
            recv_sem=tp_recv.at[d - 1],
            device_id=(sp, peer),
            device_id_type=MESH,
        )
        copy.start()
        to_heads.append(copy)
    heads[tp] = att[tp]
    hop_own(1)
    hop_far(0)
    locs["o"].wait()
    for copy in to_heads:
        copy.wait_recv()

    span = math.gcd(ow.shape[1], 512)

    def project(i, carry):
        cols = pl.ds(pl.multiple_of(i * span, span), span)
        total = jnp.zeros((rows, span), jnp.float32)
        for t in range(tn):
            total += jnp.dot(
                heads[t], ow[t * width : (t + 1) * width, cols], preferred_element_type=jnp.float32
            )
        proj[:, cols] = total
        return carry

    lax.fori_loop(0, wide // span, project, 0)
    projected = proj[...]
    middle = (
        res_ref[...].astype(jnp.float32)
        + og_ref[...]
        * (projected * lax.rsqrt(jnp.mean(projected * projected, axis=-1, keepdims=True) + EPS))
    ).astype(jnp.bfloat16)
    mid[...] = middle
    middle = middle.astype(jnp.float32)
    toks[pl.ds(pl.multiple_of(z * rows, rows), rows), :] = (
        mg_ref[...] * (middle * lax.rsqrt(jnp.mean(middle * middle, axis=-1, keepdims=True) + EPS))
    ).astype(jnp.bfloat16)

    ahead = {0: nz - 1 - z, 1: z}
    behind = {0: z, 1: nz - 1 - z}
    next_dev = {0: (lax.rem(sp + 2, n), tp), 1: (lax.rem(sp - 2 + n, n), tp)}
    side = rows // 2

    def token_copy(way, e, sub, lag):
        origin = z - (e - lag) if way == 0 else z + (e - lag)
        part = toks.at[pl.ds(pl.multiple_of(origin * rows + sub * side, 16), side), :]
        index = (way * nz + e) * 2 + sub
        return pltpu.make_async_remote_copy(
            src_ref=part,
            dst_ref=part,
            send_sem=t_send.at[index],
            recv_sem=t_recv.at[index],
            device_id=next_dev[way],
            device_id_type=MESH,
        )

    for sub in range(2):
        for way in range(2):

            @pl.when(ahead[way] > 0)
            def _():
                token_copy(way, 1, sub, 1).start()

    def token_hop(e):
        for sub in range(2):
            for way in range(2):

                @pl.when(behind[way] >= e)
                def _():
                    token_copy(way, e, sub, 0).wait_recv()

                    @pl.when(ahead[way] > 0)
                    def _():
                        token_copy(way, e + 1, sub, 1).start()

    for k in range(1, nz):
        if k > 1:
            hop_own(k)
        hop_side(k)
        if k == nz - 1:
            token_hop(1)
        hop_far(k)
    for e in range(2, nz):
        token_hop(e)
    for k in range(nz):
        for part in grain[k]:
            for kind in ("cz", "cy", "cx", "cd"):
                weight_wait(kind, k, part)

    def feed(base, size):
        branches = []
        for which in range(2):
            total = jnp.zeros((nz * rows, size), jnp.float32)
            for s in range(n):
                total += lax.dot_general(
                    toks[:, s * depth : (s + 1) * depth],
                    wall[s, which, pl.ds(base, size), :],
                    (((1,), (1,)), ((), ())),
                    preferred_element_type=jnp.float32,
                )
            branches.append(total)
        gate, up = branches
        return (gate / (1.0 + jnp.exp(-gate)) * up).astype(jnp.bfloat16)

    tile = 256

    def feed_tile(j, carry):
        base = pl.multiple_of(j * tile, tile)
        inner[:, pl.ds(base, tile)] = feed(base, tile)
        return carry

    lax.fori_loop(0, units // tile, feed_tile, 0)
    rest = units % tile
    if rest:
        inner[:, units - rest :] = feed(units - rest, rest)

    blocks = n // 2
    cut = wide // blocks

    def columns(j):
        return pl.ds(pl.multiple_of(j * cut, 128), cut)

    def sum_copy(way, d, j):
        return pltpu.make_async_remote_copy(
            src_ref=psend.at[way, d - 1, :, columns(j)],
            dst_ref=precv.at[way, d - 1, :, columns(j)],
            send_sem=p_send.at[(way * nz + d) * blocks + j],
            recv_sem=p_recv.at[(way * nz + d) * blocks + j],
            device_id=next_dev[way],
            device_id_type=MESH,
        )

    def sum_wait(way, d, j):
        sum_copy(way, d + 1, j).wait_recv()

    def share(way, d, j):
        owner = z + d if way == 0 else z - d
        return osc[pl.ds(pl.multiple_of(owner * rows, rows), rows), columns(j)]

    def down(j, carry):
        for part in range(2):
            s = 2 * j + part
            osc[:, pl.ds(pl.multiple_of(s * depth, 128), depth)] = jnp.dot(
                inner[...], wall[s, 2], preferred_element_type=jnp.float32
            )
        for way in range(2):

            @pl.when(behind[way] == 0)
            def _():
                for d in range(nz - 1, 0, -1):
                    psend[way, d - 1, :, columns(j)] = share(way, d, j).astype(jnp.bfloat16)
                    sum_copy(way, d, j).start()

        return carry

    lax.fori_loop(0, blocks, down, 0)

    def collect(j, carry):
        for d in range(nz - 2, 0, -1):
            for way in range(2):

                @pl.when(jnp.logical_and(behind[way] > 0, ahead[way] >= d))
                def _():
                    sum_wait(way, d, j)
                    psend[way, d - 1, :, columns(j)] = (
                        share(way, d, j) + precv[way, d, :, columns(j)].astype(jnp.float32)
                    ).astype(jnp.bfloat16)
                    sum_copy(way, d, j).start()

        proj[:, columns(j)] = share(0, 0, j)
        for way in range(2):

            @pl.when(behind[way] > 0)
            def _():
                sum_wait(way, 0, j)
                proj[:, columns(j)] += precv[way, 0, :, columns(j)].astype(jnp.float32)

        return carry

    lax.fori_loop(0, blocks, collect, 0)
    total = proj[...]
    out_ref[...] = (
        mid[...].astype(jnp.float32)
        + fg_ref[...] * (total * lax.rsqrt(jnp.mean(total * total, axis=-1, keepdims=True) + EPS))
    ).astype(jnp.bfloat16)
    for copy in started + to_heads:
        copy.wait_send()

    for way in range(2):
        for e in range(1, nz):

            @pl.when(jnp.logical_and(ahead[way] > 0, behind[way] >= e - 1))
            def _():
                for sub in range(2):
                    token_copy(way, e, sub, 1).wait_send()

            @pl.when(ahead[way] >= e)
            def _():
                def drain(j, carry):
                    sum_copy(way, e, j).wait_send()
                    return carry

                lax.fori_loop(0, blocks, drain, 0)


def rotary_tables(tok_rows, head_size):
    quarter = head_size // 4
    positions = lax.axis_index("sp") * tok_rows + jnp.arange(tok_rows, dtype=jnp.int32)
    lane = jnp.arange(head_size, dtype=jnp.int32)
    freqs = 10000.0 ** (-(lane % quarter).astype(jnp.float32) / quarter)
    row = (positions // GRID_W).astype(jnp.float32)[:, None]
    column = (positions % GRID_W).astype(jnp.float32)[:, None]
    angle = jnp.where(lane < 2 * quarter, row, column) * freqs
    sine = jnp.sin(angle)
    return jnp.cos(angle), jnp.where(lane % (2 * quarter) < quarter, -sine, sine)


def fused(n, tn, *args):
    (queries, keys, values, q_gain, k_gain, out_weight, out_gain, residual_in) = args[:8]
    (mlp_gain, gate_weight, up_weight, down_weight, final_gain) = args[8:]
    tok, hd = keys.shape
    groups = queries.shape[1] // hd
    depth, hidden = gate_weight.shape
    rows, wide = residual_in.shape
    cosine, sine = rotary_tables(tok, hd)
    vmem = pl.BlockSpec(memory_space=pltpu.VMEM)
    hbm = pl.BlockSpec(memory_space=pl.ANY)
    half = n // 2
    b16, f32 = jnp.bfloat16, jnp.float32
    return pl.pallas_call(
        functools.partial(layer_kernel, n, tn),
        out_shape=jax.ShapeDtypeStruct((rows, wide), b16),
        in_specs=[vmem, vmem, hbm, vmem, vmem, vmem, vmem, hbm, vmem, vmem, vmem, hbm, hbm, hbm, vmem],
        out_specs=vmem,
        scratch_shapes=[
            pltpu.VMEM((groups, hd, tok), b16),
            pltpu.VMEM((n, tok, hd), b16),
            pltpu.VMEM((n, hd, tok), b16),
            pltpu.VMEM((tok, hd), b16),
            pltpu.VMEM((2, depth, hidden), b16),
            pltpu.VMEM((3, hidden, depth), b16),
            pltpu.VMEM((n, 3, hidden // half * tn, depth), b16),
            pltpu.VMEM((wide, wide), b16),
            pltpu.VMEM((groups, 1, tok), f32),
            pltpu.VMEM((groups, 1, tok), f32),
            pltpu.VMEM((groups, hd, tok), f32),
            pltpu.VMEM((tn, rows, groups * hd), b16),
            pltpu.VMEM((tn, rows, groups * hd), b16),
            pltpu.VMEM((rows, wide), f32),
            pltpu.VMEM((rows, wide), b16),
            pltpu.VMEM((half * rows, wide), b16),
            pltpu.VMEM((half * rows, hidden // half * tn), b16),
            pltpu.VMEM((half * rows, wide), f32),
            pltpu.VMEM((2, half - 1, rows, wide), b16),
            pltpu.VMEM((2, half - 1, rows, wide), b16),
            pltpu.SemaphoreType.DMA((6,)),
            pltpu.SemaphoreType.DMA((4 * half,)),
            pltpu.SemaphoreType.DMA((4 * half,)),
            pltpu.SemaphoreType.DMA((tn - 1,)),
            pltpu.SemaphoreType.DMA((tn - 1,)),
            pltpu.SemaphoreType.DMA((8 * half * 3,)),
            pltpu.SemaphoreType.DMA((8 * half * 3,)),
            pltpu.SemaphoreType.DMA((2 * half * 2,)),
            pltpu.SemaphoreType.DMA((2 * half * 2,)),
            pltpu.SemaphoreType.DMA((2 * half * half,)),
            pltpu.SemaphoreType.DMA((2 * half * half,)),
        ],
        compiler_params=pltpu.CompilerParams(
            collective_id=0, has_side_effects=True, vmem_limit_bytes=67043328
        ),
    )(
        queries,
        keys,
        values,
        cosine,
        sine,
        q_gain[None],
        k_gain[None],
        out_weight,
        out_gain[None],
        residual_in,
        mlp_gain[None],
        gate_weight,
        up_weight,
        down_weight,
        final_gain[None],
    )


def body(mesh, *args):
    n, tn = mesh.shape["sp"], mesh.shape["tp"]
    tok, hd = args[1].shape
    depth, hidden = args[9].shape
    fits = n % 2 == 0 and 4 <= n <= 8 and depth % 128 == 0 and hidden % 128 == 0
    fits = fits and tn == 4 and hidden % (8 * n) == 0 and args[7].shape[0] % 128 == 0
    if fits and tok % 256 == 0 and hd == 128:
        return fused(n, tn, *args)
    return on_device(*args)


def solution(mesh):
    return jax.shard_map(
        functools.partial(body, mesh),
        mesh=mesh,
        in_specs=(
            P("sp", "tp"),
            P("sp", "tp"),
            P("sp", "tp"),
            P(),
            P(),
            P(),
            P(),
            P(("sp", "tp"), None),
            P(),
            P("sp", "tp"),
            P("sp", "tp"),
            P("tp", "sp"),
            P(),
        ),
        out_specs=P(("sp", "tp"), None),
        check_vma=False,
    )
```

```python
import functools
import math

import jax
import jax.numpy as jnp
from jax import lax
from jax.experimental import pallas as pl
from jax.experimental.pallas import tpu as pltpu
from jax.sharding import PartitionSpec as P

GRID_W = 64


def rms_scale(matrix):
    return matrix * lax.rsqrt(jnp.mean(matrix * matrix, axis=-1, keepdims=True) + 1e-06)


def rotary(matrix, positions):
    quarter = matrix.shape[-1] // 4
    freqs = 10000.0 ** (-jnp.arange(quarter, dtype=jnp.float32) / quarter)
    grid = jnp.stack([positions // GRID_W, positions % GRID_W], axis=-1).astype(jnp.float32)
    angle = grid[:, :, None] * freqs
    cosine = jnp.cos(angle)[:, None]
    sine = jnp.sin(angle)[:, None]
    parts = matrix.reshape(matrix.shape[:-1] + (2, 2, quarter))
    first = parts[..., 0, :]
    second = parts[..., 1, :]
    turned = jnp.stack([first * cosine - second * sine, second * cosine + first * sine], axis=-2)
    return turned.reshape(matrix.shape)


def on_device(
    queries,
    keys,
    values,
    q_gain,
    k_gain,
    out_weight,
    out_gain,
    residual_in,
    mlp_gain,
    gate_weight,
    up_weight,
    down_weight,
    final_gain,
):
    tok_rows = queries.shape[0]
    head_size = q_gain.shape[0]
    q_heads = queries.shape[1] // head_size
    kv_heads = keys.shape[1] // head_size
    group_size = q_heads // kv_heads
    positions = lax.axis_index("sp") * tok_rows + jnp.arange(tok_rows, dtype=jnp.int32)
    query_rot = rotary(
        rms_scale(queries.reshape(tok_rows, q_heads, head_size).astype(jnp.float32)) * q_gain,
        positions,
    ).astype(jnp.bfloat16)
    key_rot = rotary(
        rms_scale(keys.reshape(tok_rows, kv_heads, head_size).astype(jnp.float32)) * k_gain,
        positions,
    ).astype(jnp.bfloat16)
    key_flat = key_rot.reshape(tok_rows, kv_heads * head_size)
    grouped = query_rot.reshape(tok_rows, kv_heads, group_size, head_size)
    score_scale = head_size ** (-0.5)
    key_all, value_all = (
        lax.all_gather(key_flat, "sp", axis=0, tiled=True),
        lax.all_gather(values, "sp", axis=0, tiled=True),
    )
    total_rows = key_all.shape[0]
    span = math.gcd(total_rows, 1024)
    key_blocks = key_all.reshape(total_rows // span, span, kv_heads, head_size)
    value_blocks = value_all.reshape(total_rows // span, span, kv_heads, head_size)

    def step(run_state, blocks):
        highest, weight_sum, accum = run_state
        key_block, value_block = blocks
        scores = (
            jnp.einsum("qcgd,kcd->cgqk", grouped, key_block, preferred_element_type=jnp.float32)
            * score_scale
        )
        new_high = jnp.maximum(highest, jnp.max(scores, axis=-1))
        factor = jnp.exp(highest - new_high)
        exp_scores = jnp.exp(scores - new_high[..., None])
        weight_sum = weight_sum * factor + jnp.sum(exp_scores, axis=-1)
        accum = accum * factor[..., None] + jnp.einsum(
            "cgqk,kcd->cgqd",
            exp_scores.astype(jnp.bfloat16),
            value_block,
            preferred_element_type=jnp.float32,
        )
        return ((new_high, weight_sum, accum), None)

    start_state = (
        jnp.full((kv_heads, group_size, tok_rows), -1e30, jnp.float32),
        jnp.zeros((kv_heads, group_size, tok_rows), jnp.float32),
        jnp.zeros((kv_heads, group_size, tok_rows, head_size), jnp.float32),
    )
    final_state, unused = lax.scan(step, start_state, (key_blocks, value_blocks))
    highest, weight_sum, accum = final_state
    attended = (
        jnp.transpose(accum / weight_sum[..., None], (2, 0, 1, 3))
        .reshape(tok_rows, q_heads * head_size)
        .astype(jnp.bfloat16)
    )
    head_rows = lax.all_to_all(attended, "tp", split_axis=0, concat_axis=1, tiled=True)
    projected = jnp.dot(head_rows, out_weight, preferred_element_type=jnp.float32)
    mid_stream = (residual_in.astype(jnp.float32) + out_gain * rms_scale(projected)).astype(
        jnp.bfloat16
    )
    normed = (mlp_gain * rms_scale(mid_stream.astype(jnp.float32))).astype(jnp.bfloat16)
    mixer_in = lax.all_gather(normed, "tp", axis=0, tiled=True)
    gate_proj = jnp.dot(
        mixer_in,
        lax.all_gather(gate_weight, "sp", axis=0, tiled=True),
        preferred_element_type=jnp.float32,
    )
    up_proj = jnp.dot(
        mixer_in,
        lax.all_gather(up_weight, "sp", axis=0, tiled=True),
        preferred_element_type=jnp.float32,
    )
    down_full = lax.all_gather(down_weight, "sp", axis=1, tiled=True)
    hidden = (jax.nn.silu(gate_proj) * up_proj).astype(jnp.bfloat16)
    mlp_branch = lax.psum_scatter(
        jnp.dot(hidden, down_full, preferred_element_type=jnp.float32).astype(jnp.bfloat16),
        "tp",
        scatter_dimension=0,
        tiled=True,
    ).astype(jnp.float32)
    return (mid_stream.astype(jnp.float32) + final_gain * rms_scale(mlp_branch)).astype(
        jnp.bfloat16
    )


MESH = pl.DeviceIdType.MESH
EPS = 1e-06


def layer_kernel(
    n,
    tn,
    q_in,
    k_in,
    v_hbm,
    cos_in,
    sin_in,
    qg_ref,
    kg_ref,
    ow_hbm,
    og_ref,
    res_ref,
    mg_ref,
    gate_hbm,
    up_hbm,
    down_hbm,
    fg_ref,
    out_ref,
    cos_ref,
    sin_ref,
    qs,
    kbuf,
    vbuf,
    vraw,
    raw,
    wt,
    wall,
    ow,
    m_s,
    l_s,
    acc,
    att,
    heads,
    proj,
    mid,
    toks,
    inner,
    osc,
    psend,
    precv,
    loc_sem,
    send_sem,
    recv_sem,
    tp_send,
    tp_recv,
    w_send,
    w_recv,
    t_send,
    t_recv,
    p_send,
    p_recv,
):
    sp = lax.axis_index("sp")
    tp = lax.axis_index("tp")
    half = n // 2
    nz = n // 2

    def ring_at(pos):
        pos = lax.rem(pos + 2 * n, n)
        return jnp.where(pos < half, 2 * pos, 2 * (n - 1 - pos) + 1)

    z, y = sp // 2, lax.rem(sp, 2)
    pos = jnp.where(y == 0, z, n - 1 - z)
    right, left = ring_at(pos + 1), ring_at(pos - 1)
    other_y = 1 - y
    y_dev = (sp + 1 - 2 * y, tp)
    x_dev = (sp, lax.rem(tp + tn // 2, tn))
    c_dev = (sp, tp + 1 - 2 * lax.rem(tp, 2))
    tok, hd = k_in.shape
    groups = q_in.shape[1] // hd
    depth = gate_hbm.shape[0]
    hidden = gate_hbm.shape[1]
    rows, wide = res_ref.shape
    width = groups * hd
    hq = hidden // nz
    units = hq * tn

    barrier = pltpu.get_barrier_semaphore()
    for d in range(1, n):
        pl.semaphore_signal(
            barrier, inc=1, device_id=(lax.rem(sp + d, n), tp), device_id_type=MESH
        )
    for d in range(1, tn):
        pl.semaphore_signal(
            barrier, inc=1, device_id=(sp, lax.rem(tp + d, tn)), device_id_type=MESH
        )

    locs = {
        "v": pltpu.make_async_copy(v_hbm, vraw, loc_sem.at[0]),
        "g": pltpu.make_async_copy(gate_hbm, raw.at[0], loc_sem.at[1]),
        "u": pltpu.make_async_copy(up_hbm, raw.at[1], loc_sem.at[2]),
        "d": pltpu.make_async_copy(down_hbm, wt.at[2], loc_sem.at[3]),
        "o": pltpu.make_async_copy(ow_hbm, ow, loc_sem.at[4]),
    }
    for name in "vgudo":
        locs[name].start()

    lane = lax.broadcasted_iota(jnp.int32, (tok, hd), 1)
    quarter = hd // 4
    first = lax.rem(lane, 2 * quarter) < quarter

    def turned(x, gain):
        x = x.astype(jnp.float32)
        x = x * lax.rsqrt(jnp.mean(x * x, axis=-1, keepdims=True) + EPS) * gain
        other = jnp.where(first, pltpu.roll(x, hd - quarter, 1), pltpu.roll(x, quarter, 1))
        return (x * cos_ref[...] + other * sin_ref[...]).astype(jnp.bfloat16)

    low = lane[:GRID_W] < 2 * quarter
    grid_rows = tok // GRID_W
    for row in range(grid_rows):
        part = slice(row * GRID_W, (row + 1) * GRID_W)
        for small, large in ((cos_in, cos_ref), (sin_in, sin_ref)):
            large[part, :] = jnp.where(low, small[row : row + 1, :], small[grid_rows:, :])
    kbuf[sp] = turned(k_in[...], kg_ref[...])

    pl.semaphore_wait(barrier, n - 1 + tn - 1)

    started = []

    def start(copy):
        copy.start()
        started.append(copy)

    items = {
        "k": (0, half, lambda s: kbuf.at[s]),
        "v": (1, half - 1, lambda s: vbuf.at[s]),
    }

    def ring_copy(name, way, step, origin):
        number, to_right, view = items[name]
        index = (number * 2 + way) * half + step - 1
        return pltpu.make_async_remote_copy(
            src_ref=view(origin),
            dst_ref=view(origin),
            send_sem=send_sem.at[index],
            recv_sem=recv_sem.at[index],
            device_id=(right if way == 0 else left, tp),
            device_id_type=MESH,
        )

    def counts(name):
        to_right = items[name][1]
        return ((0, to_right), (1, n - 1 - to_right))

    def send(name):
        for way, count in counts(name):
            start(ring_copy(name, way, 1, sp))

    def arrive(name, step):
        for way, count in counts(name):
            if step > count:
                continue
            origin = ring_at(pos - step) if way == 0 else ring_at(pos + step)
            ring_copy(name, way, step, origin).wait_recv()
            if step < count:
                start(ring_copy(name, way, step + 1, origin))

    bases = {"z": 0, "x": 1, "y": 2, "d": 3, "cz": 4, "cy": 5, "cx": 6, "cd": 7}
    whole = [(0, 3)]
    thirds = [(0, 1), (1, 1), (2, 1)]

    def parts(kind, k):
        return thirds if k == nz - 1 or kind == "z" or (k == 0 and kind in ("y", "d")) else whole

    def column(k, side):
        return 2 * lax.rem(z + k, nz) + side

    def piece(slot, r, part):
        return wall.at[slot, part[0] : part[0] + part[1], r * hq : (r + 1) * hq, :]

    def weight_copy(kind, k, part):
        index = (bases[kind] * nz + k) * 3 + part[0]
        if kind == "x":
            slot, r_from, r_to, dev = column(k, y), 0, 2, x_dev
        elif kind == "y":
            slot, r_from, r_to, dev = column(k, y), 0, 0, y_dev
        elif kind == "d" and k % 2 == 0:
            slot, r_from, r_to, dev = column(k, other_y), 0, 2, x_dev
        elif kind == "d":
            slot, r_from, r_to, dev = column(k, y), 2, 2, y_dev
        else:
            r_from = 0 if kind in ("cz", "cy") else 2
            r_to, dev = r_from + 1, c_dev
            slot = column(k, y if kind in ("cz", "cx") else other_y)
        return pltpu.make_async_remote_copy(
            src_ref=piece(slot, r_from, part),
            dst_ref=piece(slot, r_to, part),
            send_sem=w_send.at[index],
            recv_sem=w_recv.at[index],
            device_id=dev,
            device_id_type=MESH,
        )

    def weight_wait(kind, k, part):
        side = y if kind in ("z", "x", "cz", "cx") else other_y
        r = {"z": 0, "y": 0, "x": 2, "d": 2, "cz": 1, "cy": 1, "cx": 3, "cd": 3}[kind]
        for small in parts(kind, k):
            if small[0] < part[0] or small[0] >= part[0] + part[1]:
                continue
            index = (bases[kind] * nz + k) * 3 + small[0]
            here = piece(column(k, side), r, small)
            pltpu.make_async_remote_copy(
                src_ref=here,
                dst_ref=here,
                send_sem=w_send.at[index],
                recv_sem=w_recv.at[index],
                device_id=c_dev,
                device_id_type=MESH,
            ).wait_recv()

    spread_list = [(k, which) for k in range(1, nz) for which in range(3)]

    def spread(count):
        for k, which in spread_list[:count]:
            target = lax.rem(z - k + nz, nz)
            index = (bases["z"] * nz + k) * 3 + which
            start(
                pltpu.make_async_remote_copy(
                    src_ref=wt.at[
                        which : which + 1, pl.ds(pl.multiple_of(target * hq, 16), hq), :
                    ],
                    dst_ref=wall.at[sp, which : which + 1, 0:hq, :],
                    send_sem=w_send.at[index],
                    recv_sem=w_recv.at[index],
                    device_id=(2 * target + y, tp),
                    device_id_type=MESH,
                )
            )
        del spread_list[:count]

    def hop_own(k, kinds=("y", "x", "cz")):
        for part in thirds if k == nz - 1 else whole:
            if k > 0:
                weight_wait("z", k, part)
            for kind in kinds:
                start(weight_copy(kind, k, part))

    def hop_side(k):
        for part in thirds if k == nz - 1 else whole:
            for kind, odd in (("y", 0), ("x", 1)):
                weight_wait(kind, k, part)
                if k % 2 == odd:
                    start(weight_copy("d", k, part))
                start(weight_copy("c" + kind, k, part))

    def hop_far(k):
        for part in thirds if k == nz - 1 else whole:
            weight_wait("d", k, part)
            start(weight_copy("cd", k, part))

    send("k")
    locs["v"].wait()
    vbuf[sp] = vraw[...].T
    send("v")
    locs["g"].wait()
    locs["u"].wait()

    def transpose(i, carry):
        part = pl.ds(pl.multiple_of(i * 128, 128), 128)
        for which in range(2):
            wt[which, part, :] = raw[which, :, part].T
        return carry

    lax.fori_loop(0, hidden // 128, transpose, 0)
    locs["d"].wait()
    own_piece = pltpu.make_async_copy(
        wt.at[:, pl.ds(pl.multiple_of(z * hq, 16), hq), :], wall.at[sp, :, 0:hq, :], loc_sem.at[5]
    )
    own_piece.start()
    spread(1)
    own_piece.wait()
    hop_own(0, ("x", "cz"))
    start(weight_copy("y", 0, thirds[0]))

    for h in range(groups):
        qs[h] = turned(q_in[:, h * hd : (h + 1) * hd], qg_ref[...]).T
    m_s[...] = jnp.full_like(m_s, -1e30)
    l_s[...] = jnp.zeros_like(l_s)
    acc[...] = jnp.zeros_like(acc)
    factor = hd ** (-0.5) * math.log2(math.e)

    def attend(slots):
        def one(i, carry):
            slot = slots[0]
            if len(slots) > 1:
                slot = jnp.where(i == 0, slots[0], slots[1])
            for h in range(groups):
                scores = jnp.dot(kbuf[slot], qs[h], preferred_element_type=jnp.float32)
                before = m_s[h]
                highest = jnp.maximum(before, jnp.max(scores, axis=0, keepdims=True))
                scale = jnp.exp2((before - highest) * factor)
                probs = jnp.exp2((scores - highest) * factor)
                m_s[h] = highest
                l_s[h] = l_s[h] * scale + jnp.sum(probs, axis=0, keepdims=True)
                acc[h] = acc[h] * scale + jnp.dot(
                    vbuf[slot], probs.astype(jnp.bfloat16), preferred_element_type=jnp.float32
                )
            return carry

        lax.fori_loop(0, len(slots), one, 0)

    attend([sp])
    for step in range(1, half + 1):
        arrive("k", step)
        arrive("v", step)
        spread(1 if step < half - 1 else len(spread_list))
        if step < 3:
            start(weight_copy("y", 0, thirds[step]))
        if step <= 3:
            weight_wait("y", 0, thirds[step - 1])
            start(weight_copy("d", 0, thirds[step - 1]))
        if step == half - 1:
            start(weight_copy("cy", 0, whole[0]))
            weight_wait("x", 0, whole[0])
            start(weight_copy("cx", 0, whole[0]))
            hop_own(1)
        ends = [ring_at(pos - step), ring_at(pos + step)]
        attend(ends if step < half else ends[:1])

    for h in range(groups):
        done = (acc[h] / l_s[h]).astype(jnp.bfloat16)
        for t in range(tn):
            att[t, :, h * hd : (h + 1) * hd] = done[:, t * rows : (t + 1) * rows].T
    to_heads = []
    for d in range(1, tn):
        peer = lax.rem(tp + d, tn)
        copy = pltpu.make_async_remote_copy(
            src_ref=att.at[peer],
            dst_ref=heads.at[tp],
            send_sem=tp_send.at[d - 1],
            recv_sem=tp_recv.at[d - 1],
            device_id=(sp, peer),
            device_id_type=MESH,
        )
        copy.start()
        to_heads.append(copy)
    heads[tp] = att[tp]
    hop_far(0)
    hop_side(1)
    locs["o"].wait()
    for copy in to_heads:
        copy.wait_recv()

    span = math.gcd(ow.shape[1], 512)

    def project(i, carry):
        cols = pl.ds(pl.multiple_of(i * span, span), span)
        total = jnp.zeros((rows, span), jnp.float32)
        for t in range(tn):
            total += jnp.dot(
                heads[t], ow[t * width : (t + 1) * width, cols], preferred_element_type=jnp.float32
            )
        proj[:, cols] = total
        return carry

    lax.fori_loop(0, wide // span, project, 0)
    projected = proj[...]
    middle = (
        res_ref[...].astype(jnp.float32)
        + og_ref[...]
        * (projected * lax.rsqrt(jnp.mean(projected * projected, axis=-1, keepdims=True) + EPS))
    ).astype(jnp.bfloat16)
    mid[...] = middle
    middle = middle.astype(jnp.float32)
    normed = (
        mg_ref[...] * (middle * lax.rsqrt(jnp.mean(middle * middle, axis=-1, keepdims=True) + EPS))
    ).astype(jnp.bfloat16)

    ahead = {0: nz - 1 - z, 1: z}
    behind = {0: z, 1: nz - 1 - z}
    next_dev = {0: (lax.rem(sp + 2, n), tp), 1: (lax.rem(sp - 2 + n, n), tp)}
    side = rows // 2

    def line_rows(at):
        return pl.ds(pl.multiple_of(at * side, 16), side)

    def token_copy(part, way, e, lag):
        origin = z - (e - lag) if way == 0 else z + (e - lag)
        block = toks.at[part, line_rows(origin), :]
        index = (part * 2 + way) * nz + e
        return pltpu.make_async_remote_copy(
            src_ref=block,
            dst_ref=block,
            send_sem=t_send.at[index],
            recv_sem=t_recv.at[index],
            device_id=next_dev[way],
            device_id_type=MESH,
        )

    for part in range(2):
        toks[part, line_rows(z), :] = normed[part * side : (part + 1) * side]
    for part in range(2):
        for way in range(2):

            @pl.when(ahead[way] > 0)
            def _():
                token_copy(part, way, 1, 1).start()

    def token_hop(part, e):
        for way in range(2):

            @pl.when(behind[way] >= e)
            def _():
                token_copy(part, way, e, 0).wait_recv()

                @pl.when(ahead[way] > 0)
                def _():
                    token_copy(part, way, e + 1, 1).start()

    def weights_in():
        for k in range(nz):
            for kind in ("cz", "cy", "cx", "cd"):
                weight_wait(kind, k, (0, 3))

    def feed(part):
        def feed_tile(r, carry):
            base = pl.multiple_of(r * hq, 16)
            branches = []
            for which in range(2):
                total = jnp.zeros((hq, nz * side), jnp.float32)
                for s in range(n):
                    total += lax.dot_general(
                        wall[s, which, pl.ds(base, hq), :],
                        toks[part, :, s * depth : (s + 1) * depth],
                        (((1,), (1,)), ((), ())),
                        preferred_element_type=jnp.float32,
                    )
                branches.append(total)
            gate, up = branches
            inner[pl.ds(base, hq), :] = (gate / (1.0 + jnp.exp(-gate)) * up).astype(jnp.bfloat16)
            return carry

        lax.fori_loop(0, tn, feed_tile, 0)

    blocks = 2
    cut = wide // blocks

    def columns(j):
        return pl.ds(pl.multiple_of(j * cut, 128), cut)

    def sum_copy(part, way, d, j):
        index = ((part * 2 + way) * nz + d) * blocks + j
        return pltpu.make_async_remote_copy(
            src_ref=psend.at[part, way, d - 1, :, columns(j)],
            dst_ref=precv.at[part, way, d - 1, :, columns(j)],
            send_sem=p_send.at[index],
            recv_sem=p_recv.at[index],
            device_id=next_dev[way],
            device_id_type=MESH,
        )

    def sum_wait(part, way, d, j):
        sum_copy(part, way, d + 1, j).wait_recv()

    def share(part, way, d, j):
        owner = z + d if way == 0 else z - d
        return osc[part, line_rows(owner), columns(j)]

    def down(part):
        def down_block(j, carry):
            for which in range(cut // depth):
                s = (cut // depth) * j + which
                osc[part, :, pl.ds(pl.multiple_of(s * depth, 128), depth)] = lax.dot_general(
                    inner[...],
                    wall[s, 2],
                    (((0,), (0,)), ((), ())),
                    preferred_element_type=jnp.float32,
                )
            for way in range(2):

                @pl.when(behind[way] == 0)
                def _():
                    for d in range(nz - 1, 0, -1):
                        psend[part, way, d - 1, :, columns(j)] = share(part, way, d, j).astype(
                            jnp.bfloat16
                        )
                        sum_copy(part, way, d, j).start()

            return carry

        lax.fori_loop(0, blocks, down_block, 0)

    def collect(part):
        mine = slice(part * side, (part + 1) * side)

        def collect_block(j, carry):
            for d in range(nz - 2, 0, -1):
                for way in range(2):

                    @pl.when(jnp.logical_and(behind[way] > 0, ahead[way] >= d))
                    def _():
                        sum_wait(part, way, d, j)
                        psend[part, way, d - 1, :, columns(j)] = (
                            share(part, way, d, j)
                            + precv[part, way, d, :, columns(j)].astype(jnp.float32)
                        ).astype(jnp.bfloat16)
                        sum_copy(part, way, d, j).start()

            proj[mine, columns(j)] = share(part, 0, 0, j)
            for way in range(2):

                @pl.when(behind[way] > 0)
                def _():
                    sum_wait(part, way, 0, j)
                    proj[mine, columns(j)] += precv[part, way, 0, :, columns(j)].astype(jnp.float32)

            return carry

        lax.fori_loop(0, blocks, collect_block, 0)
        total = proj[mine]
        out_ref[mine] = (
            mid[mine].astype(jnp.float32)
            + fg_ref[...] * (total * lax.rsqrt(jnp.mean(total * total, axis=-1, keepdims=True) + EPS))
        ).astype(jnp.bfloat16)

    hop_far(1)
    hop_own(2)
    token_hop(0, 1)
    hop_own(3)
    hop_side(2)
    token_hop(1, 1)
    token_hop(0, 2)
    hop_side(3)
    token_hop(1, 2)
    token_hop(0, 3)
    hop_far(2)
    hop_far(3)
    weights_in()
    feed(0)
    down(0)
    token_hop(1, 3)
    feed(1)
    down(1)
    collect(0)
    collect(1)
    for copy in started + to_heads:
        copy.wait_send()

    for part in range(2):
        for way in range(2):
            for e in range(1, nz):

                @pl.when(jnp.logical_and(ahead[way] > 0, behind[way] >= e - 1))
                def _():
                    token_copy(part, way, e, 1).wait_send()

                @pl.when(ahead[way] >= e)
                def _():
                    def drain(j, carry):
                        sum_copy(part, way, e, j).wait_send()
                        return carry

                    lax.fori_loop(0, blocks, drain, 0)


def rotary_tables(tok_rows, head_size):
    quarter = head_size // 4
    grid_rows = tok_rows // GRID_W
    lane = jnp.arange(head_size, dtype=jnp.int32)
    freqs = 10000.0 ** (-(lane % quarter).astype(jnp.float32) / quarter)
    index = jnp.arange(grid_rows + GRID_W, dtype=jnp.int32)
    base = lax.axis_index("sp") * grid_rows
    place = jnp.where(index < grid_rows, base + index, index - grid_rows)
    angle = place.astype(jnp.float32)[:, None] * freqs
    sine = jnp.sin(angle)
    return jnp.cos(angle), jnp.where(lane % (2 * quarter) < quarter, -sine, sine)


def fused(n, tn, *args):
    (queries, keys, values, q_gain, k_gain, out_weight, out_gain, residual_in) = args[:8]
    (mlp_gain, gate_weight, up_weight, down_weight, final_gain) = args[8:]
    tok, hd = keys.shape
    groups = queries.shape[1] // hd
    depth, hidden = gate_weight.shape
    rows, wide = residual_in.shape
    cosine, sine = rotary_tables(tok, hd)
    vmem = pl.BlockSpec(memory_space=pltpu.VMEM)
    hbm = pl.BlockSpec(memory_space=pl.ANY)
    half = n // 2
    b16, f32 = jnp.bfloat16, jnp.float32
    return pl.pallas_call(
        functools.partial(layer_kernel, n, tn),
        out_shape=jax.ShapeDtypeStruct((rows, wide), b16),
        in_specs=[vmem, vmem, hbm, vmem, vmem, vmem, vmem, hbm, vmem, vmem, vmem, hbm, hbm, hbm, vmem],
        out_specs=vmem,
        scratch_shapes=[
            pltpu.VMEM((tok, hd), f32),
            pltpu.VMEM((tok, hd), f32),
            pltpu.VMEM((groups, hd, tok), b16),
            pltpu.VMEM((n, tok, hd), b16),
            pltpu.VMEM((n, hd, tok), b16),
            pltpu.VMEM((tok, hd), b16),
            pltpu.VMEM((2, depth, hidden), b16),
            pltpu.VMEM((3, hidden, depth), b16),
            pltpu.VMEM((n, 3, hidden // half * tn, depth), b16),
            pltpu.VMEM((wide, wide), b16),
            pltpu.VMEM((groups, 1, tok), f32),
            pltpu.VMEM((groups, 1, tok), f32),
            pltpu.VMEM((groups, hd, tok), f32),
            pltpu.VMEM((tn, rows, groups * hd), b16),
            pltpu.VMEM((tn, rows, groups * hd), b16),
            pltpu.VMEM((rows, wide), f32),
            pltpu.VMEM((rows, wide), b16),
            pltpu.VMEM((2, half * rows // 2, wide), b16),
            pltpu.VMEM((hidden // half * tn, half * rows // 2), b16),
            pltpu.VMEM((2, half * rows // 2, wide), f32),
            pltpu.VMEM((2, 2, half - 1, rows // 2, wide), b16),
            pltpu.VMEM((2, 2, half - 1, rows // 2, wide), b16),
            pltpu.SemaphoreType.DMA((6,)),
            pltpu.SemaphoreType.DMA((4 * half,)),
            pltpu.SemaphoreType.DMA((4 * half,)),
            pltpu.SemaphoreType.DMA((tn - 1,)),
            pltpu.SemaphoreType.DMA((tn - 1,)),
            pltpu.SemaphoreType.DMA((8 * half * 3,)),
            pltpu.SemaphoreType.DMA((8 * half * 3,)),
            pltpu.SemaphoreType.DMA((2 * half * 2,)),
            pltpu.SemaphoreType.DMA((2 * half * 2,)),
            pltpu.SemaphoreType.DMA((8 * half,)),
            pltpu.SemaphoreType.DMA((8 * half,)),
        ],
        compiler_params=pltpu.CompilerParams(
            collective_id=0, has_side_effects=True, vmem_limit_bytes=67043328
        ),
    )(
        queries,
        keys,
        values,
        cosine,
        sine,
        q_gain[None],
        k_gain[None],
        out_weight,
        out_gain[None],
        residual_in,
        mlp_gain[None],
        gate_weight,
        up_weight,
        down_weight,
        final_gain[None],
    )


def body(mesh, *args):
    n, tn = mesh.shape["sp"], mesh.shape["tp"]
    tok, hd = args[1].shape
    depth, hidden = args[9].shape
    fits = n % 2 == 0 and n == 8 and depth % 128 == 0 and hidden % 128 == 0
    fits = fits and tn == 4 and hidden % (8 * n) == 0 and args[7].shape[0] % 128 == 0
    if fits and tok % 256 == 0 and hd == 128:
        return fused(n, tn, *args)
    return on_device(*args)


def solution(mesh):
    return jax.shard_map(
        functools.partial(body, mesh),
        mesh=mesh,
        in_specs=(
            P("sp", "tp"),
            P("sp", "tp"),
            P("sp", "tp"),
            P(),
            P(),
            P(),
            P(),
            P(("sp", "tp"), None),
            P(),
            P("sp", "tp"),
            P("sp", "tp"),
            P("tp", "sp"),
            P(),
        ),
        out_specs=P(("sp", "tp"), None),
        check_vma=False,
    )
```

```python
import functools
import math

import jax
import jax.numpy as jnp
from jax import lax
from jax.experimental import pallas as pl
from jax.experimental.pallas import tpu as pltpu
from jax.sharding import PartitionSpec as P

GRID_W = 64


def rms_scale(matrix):
    return matrix * lax.rsqrt(jnp.mean(matrix * matrix, axis=-1, keepdims=True) + 1e-06)


def rotary(matrix, positions):
    quarter = matrix.shape[-1] // 4
    freqs = 10000.0 ** (-jnp.arange(quarter, dtype=jnp.float32) / quarter)
    grid = jnp.stack([positions // GRID_W, positions % GRID_W], axis=-1).astype(jnp.float32)
    angle = grid[:, :, None] * freqs
    cosine = jnp.cos(angle)[:, None]
    sine = jnp.sin(angle)[:, None]
    parts = matrix.reshape(matrix.shape[:-1] + (2, 2, quarter))
    first = parts[..., 0, :]
    second = parts[..., 1, :]
    turned = jnp.stack([first * cosine - second * sine, second * cosine + first * sine], axis=-2)
    return turned.reshape(matrix.shape)


def on_device(
    queries,
    keys,
    values,
    q_gain,
    k_gain,
    out_weight,
    out_gain,
    residual_in,
    mlp_gain,
    gate_weight,
    up_weight,
    down_weight,
    final_gain,
):
    tok_rows = queries.shape[0]
    head_size = q_gain.shape[0]
    q_heads = queries.shape[1] // head_size
    kv_heads = keys.shape[1] // head_size
    group_size = q_heads // kv_heads
    positions = lax.axis_index("sp") * tok_rows + jnp.arange(tok_rows, dtype=jnp.int32)
    query_rot = rotary(
        rms_scale(queries.reshape(tok_rows, q_heads, head_size).astype(jnp.float32)) * q_gain,
        positions,
    ).astype(jnp.bfloat16)
    key_rot = rotary(
        rms_scale(keys.reshape(tok_rows, kv_heads, head_size).astype(jnp.float32)) * k_gain,
        positions,
    ).astype(jnp.bfloat16)
    key_flat = key_rot.reshape(tok_rows, kv_heads * head_size)
    grouped = query_rot.reshape(tok_rows, kv_heads, group_size, head_size)
    score_scale = head_size ** (-0.5)
    key_all, value_all = (
        lax.all_gather(key_flat, "sp", axis=0, tiled=True),
        lax.all_gather(values, "sp", axis=0, tiled=True),
    )
    total_rows = key_all.shape[0]
    span = math.gcd(total_rows, 1024)
    key_blocks = key_all.reshape(total_rows // span, span, kv_heads, head_size)
    value_blocks = value_all.reshape(total_rows // span, span, kv_heads, head_size)

    def step(run_state, blocks):
        highest, weight_sum, accum = run_state
        key_block, value_block = blocks
        scores = (
            jnp.einsum("qcgd,kcd->cgqk", grouped, key_block, preferred_element_type=jnp.float32)
            * score_scale
        )
        new_high = jnp.maximum(highest, jnp.max(scores, axis=-1))
        factor = jnp.exp(highest - new_high)
        exp_scores = jnp.exp(scores - new_high[..., None])
        weight_sum = weight_sum * factor + jnp.sum(exp_scores, axis=-1)
        accum = accum * factor[..., None] + jnp.einsum(
            "cgqk,kcd->cgqd",
            exp_scores.astype(jnp.bfloat16),
            value_block,
            preferred_element_type=jnp.float32,
        )
        return ((new_high, weight_sum, accum), None)

    start_state = (
        jnp.full((kv_heads, group_size, tok_rows), -1e30, jnp.float32),
        jnp.zeros((kv_heads, group_size, tok_rows), jnp.float32),
        jnp.zeros((kv_heads, group_size, tok_rows, head_size), jnp.float32),
    )
    final_state, unused = lax.scan(step, start_state, (key_blocks, value_blocks))
    highest, weight_sum, accum = final_state
    attended = (
        jnp.transpose(accum / weight_sum[..., None], (2, 0, 1, 3))
        .reshape(tok_rows, q_heads * head_size)
        .astype(jnp.bfloat16)
    )
    head_rows = lax.all_to_all(attended, "tp", split_axis=0, concat_axis=1, tiled=True)
    projected = jnp.dot(head_rows, out_weight, preferred_element_type=jnp.float32)
    mid_stream = (residual_in.astype(jnp.float32) + out_gain * rms_scale(projected)).astype(
        jnp.bfloat16
    )
    normed = (mlp_gain * rms_scale(mid_stream.astype(jnp.float32))).astype(jnp.bfloat16)
    mixer_in = lax.all_gather(normed, "tp", axis=0, tiled=True)
    gate_proj = jnp.dot(
        mixer_in,
        lax.all_gather(gate_weight, "sp", axis=0, tiled=True),
        preferred_element_type=jnp.float32,
    )
    up_proj = jnp.dot(
        mixer_in,
        lax.all_gather(up_weight, "sp", axis=0, tiled=True),
        preferred_element_type=jnp.float32,
    )
    down_full = lax.all_gather(down_weight, "sp", axis=1, tiled=True)
    hidden = (jax.nn.silu(gate_proj) * up_proj).astype(jnp.bfloat16)
    mlp_branch = lax.psum_scatter(
        jnp.dot(hidden, down_full, preferred_element_type=jnp.float32).astype(jnp.bfloat16),
        "tp",
        scatter_dimension=0,
        tiled=True,
    ).astype(jnp.float32)
    return (mid_stream.astype(jnp.float32) + final_gain * rms_scale(mlp_branch)).astype(
        jnp.bfloat16
    )


MESH = pl.DeviceIdType.MESH
EPS = 1e-06


def layer_kernel(
    n,
    tn,
    q_in,
    k_in,
    v_hbm,
    cos_in,
    sin_in,
    qg_ref,
    kg_ref,
    ow_hbm,
    og_ref,
    res_ref,
    mg_ref,
    gate_hbm,
    up_hbm,
    down_hbm,
    fg_ref,
    out_hbm,
    out_ref,
    cos_ref,
    sin_ref,
    qs,
    kbuf,
    vbuf,
    vraw,
    raw,
    wt,
    wall,
    ow,
    m_s,
    l_s,
    acc,
    att,
    heads,
    proj,
    mid,
    toks,
    inner,
    osc,
    psend,
    precv,
    loc_sem,
    send_sem,
    recv_sem,
    tp_send,
    tp_recv,
    w_send,
    w_recv,
    t_send,
    t_recv,
    p_send,
    p_recv,
):
    sp = lax.axis_index("sp")
    tp = lax.axis_index("tp")
    half = n // 2
    nz = n // 2

    def ring_at(pos):
        pos = lax.rem(pos + 2 * n, n)
        return jnp.where(pos < half, 2 * pos, 2 * (n - 1 - pos) + 1)

    z, y = sp // 2, lax.rem(sp, 2)
    pos = jnp.where(y == 0, z, n - 1 - z)
    right, left = ring_at(pos + 1), ring_at(pos - 1)
    other_y = 1 - y
    y_dev = (sp + 1 - 2 * y, tp)
    x_dev = (sp, lax.rem(tp + tn // 2, tn))
    c_dev = (sp, tp + 1 - 2 * lax.rem(tp, 2))
    tok, hd = k_in.shape
    groups = q_in.shape[1] // hd
    depth = gate_hbm.shape[0]
    hidden = gate_hbm.shape[1]
    rows, wide = res_ref.shape
    width = groups * hd
    hq = hidden // nz
    units = hq * tn

    barrier = pltpu.get_barrier_semaphore()
    for d in range(1, n):
        pl.semaphore_signal(
            barrier, inc=1, device_id=(lax.rem(sp + d, n), tp), device_id_type=MESH
        )
    for d in range(1, tn):
        pl.semaphore_signal(
            barrier, inc=1, device_id=(sp, lax.rem(tp + d, tn)), device_id_type=MESH
        )

    locs = {
        "v": pltpu.make_async_copy(v_hbm, vraw, loc_sem.at[0]),
        "g": pltpu.make_async_copy(gate_hbm, raw.at[0], loc_sem.at[1]),
        "u": pltpu.make_async_copy(up_hbm, raw.at[1], loc_sem.at[2]),
        "d": pltpu.make_async_copy(down_hbm, wt.at[2], loc_sem.at[3]),
        "o": pltpu.make_async_copy(ow_hbm, ow, loc_sem.at[4]),
    }
    for name in "vgudo":
        locs[name].start()

    lane = lax.broadcasted_iota(jnp.int32, (tok, hd), 1)
    quarter = hd // 4
    first = lax.rem(lane, 2 * quarter) < quarter

    def turned(x, gain):
        x = x.astype(jnp.float32)
        x = x * lax.rsqrt(jnp.mean(x * x, axis=-1, keepdims=True) + EPS) * gain
        other = jnp.where(first, pltpu.roll(x, hd - quarter, 1), pltpu.roll(x, quarter, 1))
        return (x * cos_ref[...] + other * sin_ref[...]).astype(jnp.bfloat16)

    low = lane[:GRID_W] < 2 * quarter
    grid_rows = tok // GRID_W
    for row in range(grid_rows):
        part = slice(row * GRID_W, (row + 1) * GRID_W)
        for small, large in ((cos_in, cos_ref), (sin_in, sin_ref)):
            large[part, :] = jnp.where(low, small[row : row + 1, :], small[grid_rows:, :])
    kbuf[sp] = turned(k_in[...], kg_ref[...])

    pl.semaphore_wait(barrier, n - 1 + tn - 1)

    started = []

    def start(copy):
        copy.start()
        started.append(copy)

    items = {
        "k": (0, half, lambda s: kbuf.at[s]),
        "v": (1, half - 1, lambda s: vbuf.at[s]),
    }

    def ring_copy(name, way, step, origin):
        number, to_right, view = items[name]
        index = (number * 2 + way) * half + step - 1
        return pltpu.make_async_remote_copy(
            src_ref=view(origin),
            dst_ref=view(origin),
            send_sem=send_sem.at[index],
            recv_sem=recv_sem.at[index],
            device_id=(right if way == 0 else left, tp),
            device_id_type=MESH,
        )

    def counts(name):
        to_right = items[name][1]
        return ((0, to_right), (1, n - 1 - to_right))

    def send(name):
        for way, count in counts(name):
            start(ring_copy(name, way, 1, sp))

    def arrive(name, step):
        for way, count in counts(name):
            if step > count:
                continue
            origin = ring_at(pos - step) if way == 0 else ring_at(pos + step)
            ring_copy(name, way, step, origin).wait_recv()
            if step < count:
                start(ring_copy(name, way, step + 1, origin))

    bases = {"z": 0, "x": 1, "y": 2, "d": 3, "cz": 4, "cy": 5, "cx": 6, "cd": 7}
    whole = [(0, 3)]
    thirds = [(0, 1), (1, 1), (2, 1)]

    def parts(kind, k):
        return thirds if k > 0 or kind in ("y", "d") else whole

    def diagonal(k, which):
        return "x" if k == 0 or (k > 1 and which != 1) else "y"

    def column(k, side):
        return 2 * lax.rem(z + k, nz) + side

    def piece(slot, r, part):
        return wall.at[slot, part[0] : part[0] + part[1], r * hq : (r + 1) * hq, :]

    def weight_copy(kind, k, part):
        index = (bases[kind] * nz + k) * 3 + part[0]
        if kind == "x":
            slot, r_from, r_to, dev = column(k, y), 0, 2, x_dev
        elif kind == "y":
            slot, r_from, r_to, dev = column(k, y), 0, 0, y_dev
        elif kind == "d" and diagonal(k, part[0]) == "x":
            slot, r_from, r_to, dev = column(k, other_y), 0, 2, x_dev
        elif kind == "d":
            slot, r_from, r_to, dev = column(k, y), 2, 2, y_dev
        else:
            r_from = 0 if kind in ("cz", "cy") else 2
            r_to, dev = r_from + 1, c_dev
            slot = column(k, y if kind in ("cz", "cx") else other_y)
        return pltpu.make_async_remote_copy(
            src_ref=piece(slot, r_from, part),
            dst_ref=piece(slot, r_to, part),
            send_sem=w_send.at[index],
            recv_sem=w_recv.at[index],
            device_id=dev,
            device_id_type=MESH,
        )

    def weight_wait(kind, k, part):
        side = y if kind in ("z", "x", "cz", "cx") else other_y
        r = {"z": 0, "y": 0, "x": 2, "d": 2, "cz": 1, "cy": 1, "cx": 3, "cd": 3}[kind]
        for small in parts(kind, k):
            if small[0] < part[0] or small[0] >= part[0] + part[1]:
                continue
            index = (bases[kind] * nz + k) * 3 + small[0]
            here = piece(column(k, side), r, small)
            pltpu.make_async_remote_copy(
                src_ref=here,
                dst_ref=here,
                send_sem=w_send.at[index],
                recv_sem=w_recv.at[index],
                device_id=c_dev,
                device_id_type=MESH,
            ).wait_recv()

    spread_list = [(k, which) for k in (1, 3, 2) for which in range(3)]

    def spread(count):
        for k, which in spread_list[:count]:
            target = lax.rem(z - k + nz, nz)
            index = (bases["z"] * nz + k) * 3 + which
            start(
                pltpu.make_async_remote_copy(
                    src_ref=wt.at[
                        which : which + 1, pl.ds(pl.multiple_of(target * hq, 16), hq), :
                    ],
                    dst_ref=wall.at[sp, which : which + 1, 0:hq, :],
                    send_sem=w_send.at[index],
                    recv_sem=w_recv.at[index],
                    device_id=(2 * target + y, tp),
                    device_id_type=MESH,
                )
            )
        del spread_list[:count]

    def hop_own(k, some=(0, 1, 2)):
        for which in some:
            weight_wait("z", k, thirds[which])
            for kind in ("y", "x", "cz"):
                start(weight_copy(kind, k, thirds[which]))

    def hop_side(k, some=(0, 1, 2)):
        for which in some:
            for kind, route in (("y", "x"), ("x", "y")):
                weight_wait(kind, k, thirds[which])
                if diagonal(k, which) == route:
                    start(weight_copy("d", k, thirds[which]))
                start(weight_copy("c" + kind, k, thirds[which]))

    def hop_far(k, some=(0, 1, 2)):
        for which in some:
            weight_wait("d", k, thirds[which])
            if k > 0:
                start(weight_copy("cd", k, thirds[which]))
        if k == 0:
            start(weight_copy("cd", k, whole[0]))

    send("k")
    locs["v"].wait()
    vbuf[sp] = vraw[...].T
    send("v")
    locs["g"].wait()
    locs["u"].wait()

    def transpose(i, carry):
        part = pl.ds(pl.multiple_of(i * 128, 128), 128)
        for which in range(2):
            wt[which, part, :] = raw[which, :, part].T
        return carry

    lax.fori_loop(0, hidden // 128, transpose, 0)
    locs["d"].wait()
    own_piece = pltpu.make_async_copy(
        wt.at[:, pl.ds(pl.multiple_of(z * hq, 16), hq), :], wall.at[sp, :, 0:hq, :], loc_sem.at[5]
    )
    own_piece.start()
    spread(1)
    own_piece.wait()
    start(weight_copy("x", 0, whole[0]))
    start(weight_copy("cz", 0, whole[0]))
    start(weight_copy("y", 0, thirds[0]))

    for h in range(groups):
        qs[h] = turned(q_in[:, h * hd : (h + 1) * hd], qg_ref[...]).T
    m_s[...] = jnp.full_like(m_s, -1e30)
    l_s[...] = jnp.zeros_like(l_s)
    acc[...] = jnp.zeros_like(acc)
    factor = hd ** (-0.5) * math.log2(math.e)

    def attend(slots):
        def one(i, carry):
            slot = slots[0]
            if len(slots) > 1:
                slot = jnp.where(i == 0, slots[0], slots[1])
            for h in range(groups):
                scores = jnp.dot(kbuf[slot], qs[h], preferred_element_type=jnp.float32)
                before = m_s[h]
                highest = jnp.maximum(before, jnp.max(scores, axis=0, keepdims=True))
                scale = jnp.exp2((before - highest) * factor)
                probs = jnp.exp2((scores - highest) * factor)
                m_s[h] = highest
                l_s[h] = l_s[h] * scale + jnp.sum(probs, axis=0, keepdims=True)
                acc[h] = acc[h] * scale + jnp.dot(
                    vbuf[slot], probs.astype(jnp.bfloat16), preferred_element_type=jnp.float32
                )
            return carry

        lax.fori_loop(0, len(slots), one, 0)

    attend([sp])
    for step in range(1, half + 1):
        arrive("k", step)
        arrive("v", step)
        if step != half - 1:
            spread(1 if step < half else 4)
        if step < 3:
            start(weight_copy("y", 0, thirds[step]))
        if step <= 3:
            weight_wait("y", 0, thirds[step - 1])
            start(weight_copy("d", 0, thirds[step - 1]))
        if step == half - 1:
            start(weight_copy("cy", 0, whole[0]))
            weight_wait("x", 0, whole[0])
            start(weight_copy("cx", 0, whole[0]))
            hop_own(1)
        ends = [ring_at(pos - step), ring_at(pos + step)]
        attend(ends if step < half else ends[:1])

    for h in range(groups):
        done = (acc[h] / l_s[h]).astype(jnp.bfloat16)
        for t in range(tn):
            att[t, :, h * hd : (h + 1) * hd] = done[:, t * rows : (t + 1) * rows].T
    to_heads = []
    for d in range(1, tn):
        peer = lax.rem(tp + d, tn)
        copy = pltpu.make_async_remote_copy(
            src_ref=att.at[peer],
            dst_ref=heads.at[tp],
            send_sem=tp_send.at[d - 1],
            recv_sem=tp_recv.at[d - 1],
            device_id=(sp, peer),
            device_id_type=MESH,
        )
        copy.start()
        to_heads.append(copy)
    heads[tp] = att[tp]
    hop_far(0)
    hop_side(1)
    hop_own(3, (0, 1))
    locs["o"].wait()
    for copy in to_heads:
        copy.wait_recv()

    span = math.gcd(ow.shape[1], 512)

    def project(i, carry):
        cols = pl.ds(pl.multiple_of(i * span, span), span)
        total = jnp.zeros((rows, span), jnp.float32)
        for t in range(tn):
            total += jnp.dot(
                heads[t], ow[t * width : (t + 1) * width, cols], preferred_element_type=jnp.float32
            )
        proj[:, cols] = total
        return carry

    lax.fori_loop(0, wide // span, project, 0)
    projected = proj[...]
    middle = (
        res_ref[...].astype(jnp.float32)
        + og_ref[...]
        * (projected * lax.rsqrt(jnp.mean(projected * projected, axis=-1, keepdims=True) + EPS))
    ).astype(jnp.bfloat16)
    mid[...] = middle
    middle = middle.astype(jnp.float32)
    normed = (
        mg_ref[...] * (middle * lax.rsqrt(jnp.mean(middle * middle, axis=-1, keepdims=True) + EPS))
    ).astype(jnp.bfloat16)

    ahead = {0: nz - 1 - z, 1: z}
    behind = {0: z, 1: nz - 1 - z}
    next_dev = {0: (lax.rem(sp + 2, n), tp), 1: (lax.rem(sp - 2 + n, n), tp)}
    side = rows // 2

    def line_rows(at):
        return pl.ds(pl.multiple_of(at * side, 16), side)

    def token_copy(part, way, e, lag):
        origin = z - (e - lag) if way == 0 else z + (e - lag)
        block = toks.at[part, line_rows(origin), :]
        index = (part * 2 + way) * nz + e
        return pltpu.make_async_remote_copy(
            src_ref=block,
            dst_ref=block,
            send_sem=t_send.at[index],
            recv_sem=t_recv.at[index],
            device_id=next_dev[way],
            device_id_type=MESH,
        )

    for part in range(2):
        toks[part, line_rows(z), :] = normed[part * side : (part + 1) * side]
    def token_send(part):
        for way in range(2):

            @pl.when(ahead[way] > 0)
            def _():
                token_copy(part, way, 1, 1).start()

    token_send(0)

    def token_hop(part, e):
        for way in range(2):

            @pl.when(jnp.logical_and(behind[way] >= e, ahead[way] > 0))
            def _():
                token_copy(part, way, e, 0).wait_recv()
                token_copy(part, way, e + 1, 1).start()

    def tokens_in(part):
        for way in range(2):

            @pl.when(ahead[way] == 0)
            def _():
                for e in range(1, nz):
                    token_copy(part, way, e, 0).wait_recv()

    def weights_in():
        for k in range(nz):
            for kind in ("cz", "cy", "cx", "cd"):
                weight_wait(kind, k, (0, 3))

    def feed(part):
        def feed_tile(r, carry):
            base = pl.multiple_of(r * hq, 16)
            branches = []
            for which in range(2):
                total = jnp.zeros((hq, nz * side), jnp.float32)
                for s in range(n):
                    total += lax.dot_general(
                        wall[s, which, pl.ds(base, hq), :],
                        toks[part, :, s * depth : (s + 1) * depth],
                        (((1,), (1,)), ((), ())),
                        preferred_element_type=jnp.float32,
                    )
                branches.append(total)
            gate, up = branches
            inner[pl.ds(base, hq), :] = (gate / (1.0 + jnp.exp(-gate)) * up).astype(jnp.bfloat16)
            return carry

        lax.fori_loop(0, tn, feed_tile, 0)

    blocks = 1
    cut = wide // blocks

    def columns(j):
        return pl.ds(pl.multiple_of(j * cut, 128), cut)

    def sum_copy(part, way, d, j):
        index = ((part * 2 + way) * nz + d) * blocks + j
        return pltpu.make_async_remote_copy(
            src_ref=psend.at[part, way, d - 1, :, columns(j)],
            dst_ref=precv.at[part, way, d - 1, :, columns(j)],
            send_sem=p_send.at[index],
            recv_sem=p_recv.at[index],
            device_id=next_dev[way],
            device_id_type=MESH,
        )

    def sum_wait(part, way, d, j):
        sum_copy(part, way, d + 1, j).wait_recv()

    def share(part, way, d, j):
        owner = z + d if way == 0 else z - d
        return osc[part, line_rows(owner), columns(j)]

    def down(part):
        def down_block(j, carry):
            for which in range(cut // depth):
                s = (cut // depth) * j + which
                osc[part, :, pl.ds(pl.multiple_of(s * depth, 128), depth)] = lax.dot_general(
                    inner[...],
                    wall[s, 2],
                    (((0,), (0,)), ((), ())),
                    preferred_element_type=jnp.float32,
                )
            for way in range(2):

                @pl.when(behind[way] == 0)
                def _():
                    for d in range(nz - 1, 0, -1):
                        psend[part, way, d - 1, :, columns(j)] = share(part, way, d, j).astype(
                            jnp.bfloat16
                        )
                        sum_copy(part, way, d, j).start()

            return carry

        lax.fori_loop(0, blocks, down_block, 0)

    def collect(part):
        mine = slice(part * side, (part + 1) * side)

        def collect_block(j, carry):
            for d in range(nz - 2, 0, -1):
                for way in range(2):

                    @pl.when(jnp.logical_and(behind[way] > 0, ahead[way] >= d))
                    def _():
                        sum_wait(part, way, d, j)
                        psend[part, way, d - 1, :, columns(j)] = (
                            share(part, way, d, j)
                            + precv[part, way, d, :, columns(j)].astype(jnp.float32)
                        ).astype(jnp.bfloat16)
                        sum_copy(part, way, d, j).start()

            proj[mine, columns(j)] = share(part, 0, 0, j)
            for way in range(2):

                @pl.when(behind[way] > 0)
                def _():
                    sum_wait(part, way, 0, j)
                    proj[mine, columns(j)] += precv[part, way, 0, :, columns(j)].astype(jnp.float32)

            return carry

        lax.fori_loop(0, blocks, collect_block, 0)
        total = proj[mine]
        out_ref[mine] = (
            mid[mine].astype(jnp.float32)
            + fg_ref[...] * (total * lax.rsqrt(jnp.mean(total * total, axis=-1, keepdims=True) + EPS))
        ).astype(jnp.bfloat16)
        result(part).start()

    def result(part):
        mine = pl.ds(part * side, side)
        return pltpu.make_async_copy(out_ref.at[mine], out_hbm.at[mine], loc_sem.at[6 + part])

    spread(2)
    hop_own(3, (2,))
    hop_far(1)
    token_hop(0, 1)
    hop_side(3)
    hop_own(2)
    token_hop(0, 2)
    hop_side(2, (0,))
    token_send(1)
    hop_side(2, (1, 2))
    hop_far(3)
    token_hop(1, 1)
    hop_far(2)
    token_hop(1, 2)
    weights_in()
    tokens_in(0)
    feed(0)
    down(0)
    tokens_in(1)
    feed(1)
    down(1)
    collect(0)
    collect(1)
    for copy in started + to_heads:
        copy.wait_send()

    for part in range(2):
        for way in range(2):
            for e in range(1, nz):

                @pl.when(jnp.logical_and(ahead[way] > 0, behind[way] >= e - 1))
                def _():
                    token_copy(part, way, e, 1).wait_send()

                @pl.when(ahead[way] >= e)
                def _():
                    def drain(j, carry):
                        sum_copy(part, way, e, j).wait_send()
                        return carry

                    lax.fori_loop(0, blocks, drain, 0)

    for part in range(2):
        result(part).wait()


def rotary_tables(tok_rows, head_size):
    quarter = head_size // 4
    grid_rows = tok_rows // GRID_W
    lane = jnp.arange(head_size, dtype=jnp.int32)
    freqs = 10000.0 ** (-(lane % quarter).astype(jnp.float32) / quarter)
    index = jnp.arange(grid_rows + GRID_W, dtype=jnp.int32)
    base = lax.axis_index("sp") * grid_rows
    place = jnp.where(index < grid_rows, base + index, index - grid_rows)
    angle = place.astype(jnp.float32)[:, None] * freqs
    sine = jnp.sin(angle)
    return jnp.cos(angle), jnp.where(lane % (2 * quarter) < quarter, -sine, sine)


def fused(n, tn, *args):
    (queries, keys, values, q_gain, k_gain, out_weight, out_gain, residual_in) = args[:8]
    (mlp_gain, gate_weight, up_weight, down_weight, final_gain) = args[8:]
    tok, hd = keys.shape
    groups = queries.shape[1] // hd
    depth, hidden = gate_weight.shape
    rows, wide = residual_in.shape
    cosine, sine = rotary_tables(tok, hd)
    vmem = pl.BlockSpec(memory_space=pltpu.VMEM)
    hbm = pl.BlockSpec(memory_space=pl.ANY)
    half = n // 2
    b16, f32 = jnp.bfloat16, jnp.float32
    return pl.pallas_call(
        functools.partial(layer_kernel, n, tn),
        out_shape=jax.ShapeDtypeStruct((rows, wide), b16),
        in_specs=[vmem, vmem, hbm, vmem, vmem, vmem, vmem, hbm, vmem, vmem, vmem, hbm, hbm, hbm, vmem],
        out_specs=hbm,
        scratch_shapes=[
            pltpu.VMEM((rows, wide), b16),
            pltpu.VMEM((tok, hd), f32),
            pltpu.VMEM((tok, hd), f32),
            pltpu.VMEM((groups, hd, tok), b16),
            pltpu.VMEM((n, tok, hd), b16),
            pltpu.VMEM((n, hd, tok), b16),
            pltpu.VMEM((tok, hd), b16),
            pltpu.VMEM((2, depth, hidden), b16),
            pltpu.VMEM((3, hidden, depth), b16),
            pltpu.VMEM((n, 3, hidden // half * tn, depth), b16),
            pltpu.VMEM((wide, wide), b16),
            pltpu.VMEM((groups, 1, tok), f32),
            pltpu.VMEM((groups, 1, tok), f32),
            pltpu.VMEM((groups, hd, tok), f32),
            pltpu.VMEM((tn, rows, groups * hd), b16),
            pltpu.VMEM((tn, rows, groups * hd), b16),
            pltpu.VMEM((rows, wide), f32),
            pltpu.VMEM((rows, wide), b16),
            pltpu.VMEM((2, half * rows // 2, wide), b16),
            pltpu.VMEM((hidden // half * tn, half * rows // 2), b16),
            pltpu.VMEM((2, half * rows // 2, wide), f32),
            pltpu.VMEM((2, 2, half - 1, rows // 2, wide), b16),
            pltpu.VMEM((2, 2, half - 1, rows // 2, wide), b16),
            pltpu.SemaphoreType.DMA((8,)),
            pltpu.SemaphoreType.DMA((4 * half,)),
            pltpu.SemaphoreType.DMA((4 * half,)),
            pltpu.SemaphoreType.DMA((tn - 1,)),
            pltpu.SemaphoreType.DMA((tn - 1,)),
            pltpu.SemaphoreType.DMA((8 * half * 3,)),
            pltpu.SemaphoreType.DMA((8 * half * 3,)),
            pltpu.SemaphoreType.DMA((2 * half * 2,)),
            pltpu.SemaphoreType.DMA((2 * half * 2,)),
            pltpu.SemaphoreType.DMA((8 * half,)),
            pltpu.SemaphoreType.DMA((8 * half,)),
        ],
        compiler_params=pltpu.CompilerParams(
            collective_id=0, has_side_effects=True, vmem_limit_bytes=67043328
        ),
    )(
        queries,
        keys,
        values,
        cosine,
        sine,
        q_gain[None],
        k_gain[None],
        out_weight,
        out_gain[None],
        residual_in,
        mlp_gain[None],
        gate_weight,
        up_weight,
        down_weight,
        final_gain[None],
    )


def body(mesh, *args):
    n, tn = mesh.shape["sp"], mesh.shape["tp"]
    tok, hd = args[1].shape
    depth, hidden = args[9].shape
    fits = n % 2 == 0 and n == 8 and depth % 128 == 0 and hidden % 128 == 0
    fits = fits and tn == 4 and hidden % (8 * n) == 0 and args[7].shape[0] % 128 == 0
    if fits and tok % 256 == 0 and hd == 128:
        return fused(n, tn, *args)
    return on_device(*args)


def solution(mesh):
    return jax.shard_map(
        functools.partial(body, mesh),
        mesh=mesh,
        in_specs=(
            P("sp", "tp"),
            P("sp", "tp"),
            P("sp", "tp"),
            P(),
            P(),
            P(),
            P(),
            P(("sp", "tp"), None),
            P(),
            P("sp", "tp"),
            P("sp", "tp"),
            P("tp", "sp"),
            P(),
        ),
        out_specs=P(("sp", "tp"), None),
        check_vma=False,
    )
```

```python
import functools
import math

import jax
import jax.numpy as jnp
from jax import lax
from jax.experimental import pallas as pl
from jax.experimental.pallas import tpu as pltpu
from jax.sharding import PartitionSpec as P

GRID_W = 64


def rms_scale(matrix):
    return matrix * lax.rsqrt(jnp.mean(matrix * matrix, axis=-1, keepdims=True) + 1e-06)


def rotary(matrix, positions):
    quarter = matrix.shape[-1] // 4
    freqs = 10000.0 ** (-jnp.arange(quarter, dtype=jnp.float32) / quarter)
    grid = jnp.stack([positions // GRID_W, positions % GRID_W], axis=-1).astype(jnp.float32)
    angle = grid[:, :, None] * freqs
    cosine = jnp.cos(angle)[:, None]
    sine = jnp.sin(angle)[:, None]
    parts = matrix.reshape(matrix.shape[:-1] + (2, 2, quarter))
    first = parts[..., 0, :]
    second = parts[..., 1, :]
    turned = jnp.stack([first * cosine - second * sine, second * cosine + first * sine], axis=-2)
    return turned.reshape(matrix.shape)


def on_device(
    queries,
    keys,
    values,
    q_gain,
    k_gain,
    out_weight,
    out_gain,
    residual_in,
    mlp_gain,
    gate_weight,
    up_weight,
    down_weight,
    final_gain,
):
    tok_rows = queries.shape[0]
    head_size = q_gain.shape[0]
    q_heads = queries.shape[1] // head_size
    kv_heads = keys.shape[1] // head_size
    group_size = q_heads // kv_heads
    positions = lax.axis_index("sp") * tok_rows + jnp.arange(tok_rows, dtype=jnp.int32)
    query_rot = rotary(
        rms_scale(queries.reshape(tok_rows, q_heads, head_size).astype(jnp.float32)) * q_gain,
        positions,
    ).astype(jnp.bfloat16)
    key_rot = rotary(
        rms_scale(keys.reshape(tok_rows, kv_heads, head_size).astype(jnp.float32)) * k_gain,
        positions,
    ).astype(jnp.bfloat16)
    key_flat = key_rot.reshape(tok_rows, kv_heads * head_size)
    grouped = query_rot.reshape(tok_rows, kv_heads, group_size, head_size)
    score_scale = head_size ** (-0.5)
    key_all, value_all = (
        lax.all_gather(key_flat, "sp", axis=0, tiled=True),
        lax.all_gather(values, "sp", axis=0, tiled=True),
    )
    total_rows = key_all.shape[0]
    span = math.gcd(total_rows, 1024)
    key_blocks = key_all.reshape(total_rows // span, span, kv_heads, head_size)
    value_blocks = value_all.reshape(total_rows // span, span, kv_heads, head_size)

    def step(run_state, blocks):
        highest, weight_sum, accum = run_state
        key_block, value_block = blocks
        scores = (
            jnp.einsum("qcgd,kcd->cgqk", grouped, key_block, preferred_element_type=jnp.float32)
            * score_scale
        )
        new_high = jnp.maximum(highest, jnp.max(scores, axis=-1))
        factor = jnp.exp(highest - new_high)
        exp_scores = jnp.exp(scores - new_high[..., None])
        weight_sum = weight_sum * factor + jnp.sum(exp_scores, axis=-1)
        accum = accum * factor[..., None] + jnp.einsum(
            "cgqk,kcd->cgqd",
            exp_scores.astype(jnp.bfloat16),
            value_block,
            preferred_element_type=jnp.float32,
        )
        return ((new_high, weight_sum, accum), None)

    start_state = (
        jnp.full((kv_heads, group_size, tok_rows), -1e30, jnp.float32),
        jnp.zeros((kv_heads, group_size, tok_rows), jnp.float32),
        jnp.zeros((kv_heads, group_size, tok_rows, head_size), jnp.float32),
    )
    final_state, unused = lax.scan(step, start_state, (key_blocks, value_blocks))
    highest, weight_sum, accum = final_state
    attended = (
        jnp.transpose(accum / weight_sum[..., None], (2, 0, 1, 3))
        .reshape(tok_rows, q_heads * head_size)
        .astype(jnp.bfloat16)
    )
    head_rows = lax.all_to_all(attended, "tp", split_axis=0, concat_axis=1, tiled=True)
    projected = jnp.dot(head_rows, out_weight, preferred_element_type=jnp.float32)
    mid_stream = (residual_in.astype(jnp.float32) + out_gain * rms_scale(projected)).astype(
        jnp.bfloat16
    )
    normed = (mlp_gain * rms_scale(mid_stream.astype(jnp.float32))).astype(jnp.bfloat16)
    mixer_in = lax.all_gather(normed, "tp", axis=0, tiled=True)
    gate_proj = jnp.dot(
        mixer_in,
        lax.all_gather(gate_weight, "sp", axis=0, tiled=True),
        preferred_element_type=jnp.float32,
    )
    up_proj = jnp.dot(
        mixer_in,
        lax.all_gather(up_weight, "sp", axis=0, tiled=True),
        preferred_element_type=jnp.float32,
    )
    down_full = lax.all_gather(down_weight, "sp", axis=1, tiled=True)
    hidden = (jax.nn.silu(gate_proj) * up_proj).astype(jnp.bfloat16)
    mlp_branch = lax.psum_scatter(
        jnp.dot(hidden, down_full, preferred_element_type=jnp.float32).astype(jnp.bfloat16),
        "tp",
        scatter_dimension=0,
        tiled=True,
    ).astype(jnp.float32)
    return (mid_stream.astype(jnp.float32) + final_gain * rms_scale(mlp_branch)).astype(
        jnp.bfloat16
    )


MESH = pl.DeviceIdType.MESH
EPS = 1e-06


def layer_kernel(
    n,
    tn,
    q_hbm,
    k_in,
    v_hbm,
    qg_ref,
    kg_ref,
    ow_hbm,
    og_ref,
    res_hbm,
    mg_ref,
    gate_hbm,
    up_hbm,
    down_hbm,
    fg_ref,
    out_hbm,
    out_ref,
    q_in,
    res_ref,
    cos_ref,
    sin_ref,
    qs,
    kbuf,
    vbuf,
    vraw,
    raw,
    wt,
    wall,
    ow,
    m_s,
    l_s,
    acc,
    att,
    heads,
    proj,
    mid,
    toks,
    inner,
    partial,
    osc,
    psend,
    precv,
    loc_sem,
    send_sem,
    recv_sem,
    tp_send,
    tp_recv,
    w_send,
    w_recv,
    t_send,
    t_recv,
    p_send,
    p_recv,
):
    sp = lax.axis_index("sp")
    tp = lax.axis_index("tp")
    half = n // 2
    nz = n // 2

    def ring_at(pos):
        pos = lax.rem(pos + 2 * n, n)
        return jnp.where(pos < half, 2 * pos, 2 * (n - 1 - pos) + 1)

    z, y = sp // 2, lax.rem(sp, 2)
    pos = jnp.where(y == 0, z, n - 1 - z)
    right, left = ring_at(pos + 1), ring_at(pos - 1)
    other_y = 1 - y
    y_dev = (sp + 1 - 2 * y, tp)
    x_dev = (sp, lax.rem(tp + tn // 2, tn))
    c_dev = (sp, tp + 1 - 2 * lax.rem(tp, 2))
    tok, hd = k_in.shape
    groups = q_in.shape[1] // hd
    depth = gate_hbm.shape[0]
    hidden = gate_hbm.shape[1]
    rows, wide = res_ref.shape
    width = groups * hd
    hq = hidden // nz
    units = hq * tn

    barrier = pltpu.get_barrier_semaphore()
    for d in range(1, n):
        pl.semaphore_signal(
            barrier, inc=1, device_id=(lax.rem(sp + d, n), tp), device_id_type=MESH
        )
    for d in range(1, tn):
        pl.semaphore_signal(
            barrier, inc=1, device_id=(sp, lax.rem(tp + d, tn)), device_id_type=MESH
        )

    locs = {
        "v": pltpu.make_async_copy(v_hbm, vraw, loc_sem.at[0]),
        "g": pltpu.make_async_copy(gate_hbm, raw.at[0], loc_sem.at[1]),
        "u": pltpu.make_async_copy(up_hbm, raw.at[1], loc_sem.at[2]),
        "d": pltpu.make_async_copy(down_hbm, wt.at[2], loc_sem.at[3]),
        "o": pltpu.make_async_copy(ow_hbm, ow, loc_sem.at[4]),
    }
    locs["q"] = pltpu.make_async_copy(q_hbm, q_in, loc_sem.at[8])
    locs["r"] = pltpu.make_async_copy(res_hbm, res_ref, loc_sem.at[9])
    for name in "vguqdor":
        locs[name].start()

    lane = lax.broadcasted_iota(jnp.int32, (tok, hd), 1)
    quarter = hd // 4
    first = lax.rem(lane, 2 * quarter) < quarter

    def turned(x, gain):
        x = x.astype(jnp.float32)
        x = x * lax.rsqrt(jnp.mean(x * x, axis=-1, keepdims=True) + EPS) * gain
        other = jnp.where(first, pltpu.roll(x, hd - quarter, 1), pltpu.roll(x, quarter, 1))
        return (x * cos_ref[...] + other * sin_ref[...]).astype(jnp.bfloat16)

    grid_rows = tok // GRID_W
    shape = (grid_rows + GRID_W, hd)
    index = lax.broadcasted_iota(jnp.int32, shape, 0)
    spot = lax.broadcasted_iota(jnp.int32, shape, 1)
    freqs = jnp.exp(lax.rem(spot, quarter).astype(jnp.float32) * (-math.log(10000.0) / quarter))
    place = jnp.where(index < grid_rows, sp * grid_rows + index, index - grid_rows)
    angle = place.astype(jnp.float32) * freqs
    sine = jnp.sin(angle)
    turn = jnp.where(lax.rem(spot, 2 * quarter) < quarter, -sine, sine)
    low = lane[:GRID_W] < 2 * quarter
    for small, large in ((jnp.cos(angle), cos_ref), (turn, sin_ref)):
        for row in range(grid_rows):
            part = slice(row * GRID_W, (row + 1) * GRID_W)
            large[part, :] = jnp.where(low, small[row : row + 1, :], small[grid_rows:, :])
    kbuf[sp] = turned(k_in[...], kg_ref[...])

    pl.semaphore_wait(barrier, n - 1 + tn - 1)

    items = {
        "k": (0, half, lambda s: kbuf.at[s]),
        "v": (1, half - 1, lambda s: vbuf.at[s]),
    }

    def ring_copy(name, way, step, origin):
        number, to_right, view = items[name]
        index = (number * 2 + way) * half + step - 1
        return pltpu.make_async_remote_copy(
            src_ref=view(origin),
            dst_ref=view(origin),
            send_sem=send_sem.at[number],
            recv_sem=recv_sem.at[index],
            device_id=(right if way == 0 else left, tp),
            device_id_type=MESH,
        )

    def counts(name):
        to_right = items[name][1]
        return ((0, to_right), (1, n - 1 - to_right))

    def send(name):
        for way, count in counts(name):
            ring_copy(name, way, 1, sp).start()

    def arrive(name, step):
        for way, count in counts(name):
            if step > count:
                continue
            origin = ring_at(pos - step) if way == 0 else ring_at(pos + step)
            ring_copy(name, way, step, origin).wait_recv()
            if step < count:
                ring_copy(name, way, step + 1, origin).start()

    last = 2

    def w_index(kind, k, which):
        if kind[0] == "c":
            return 4 * nz * 3 + (1 if k == last else 0)
        return ("zxyd".index(kind) * nz + k) * 3 + which

    whole = [(0, 3)]
    thirds = [(0, 1), (1, 1), (2, 1)]

    def parts(kind, k):
        return thirds if k > 0 or kind in ("y", "d") else whole

    def diagonal(k, which):
        return "x" if k == 0 or (k > 1 and which != 1) else "y"

    def column(k, side):
        return 2 * lax.rem(z + k, nz) + side

    def piece(slot, r, part):
        return wall.at[slot, part[0] : part[0] + part[1], r * hq : (r + 1) * hq, :]

    def weight_copy(kind, k, part):
        if kind == "x":
            slot, r_from, r_to, dev = column(k, y), 0, 2, x_dev
        elif kind == "y":
            slot, r_from, r_to, dev = column(k, y), 0, 0, y_dev
        elif kind == "d" and diagonal(k, part[0]) == "x":
            slot, r_from, r_to, dev = column(k, other_y), 0, 2, x_dev
        elif kind == "d":
            slot, r_from, r_to, dev = column(k, y), 2, 2, y_dev
        else:
            r_from = 0 if kind in ("cz", "cy") else 2
            r_to, dev = r_from + 1, c_dev
            slot = column(k, y if kind in ("cz", "cx") else other_y)
        return pltpu.make_async_remote_copy(
            src_ref=piece(slot, r_from, part),
            dst_ref=piece(slot, r_to, part),
            send_sem=w_send.at[2 if kind[0] == "c" else 1],
            recv_sem=w_recv.at[w_index(kind, k, part[0])],
            device_id=dev,
            device_id_type=MESH,
        )

    def weight_wait(kind, k, part):
        side = y if kind in ("z", "x") else other_y
        for small in parts(kind, k):
            if small[0] < part[0] or small[0] >= part[0] + part[1]:
                continue
            here = piece(column(k, side), 0 if kind in ("z", "y") else 2, small)
            arrival(here, w_recv.at[w_index(kind, k, small[0])]).wait_recv()

    def arrival(ref, semaphore):
        return pltpu.make_async_remote_copy(
            src_ref=ref,
            dst_ref=ref,
            send_sem=semaphore,
            recv_sem=semaphore,
            device_id=c_dev,
            device_id_type=MESH,
        )

    spread_list = [(k, which) for k in (1, 3, 2) for which in range(3)]

    def spread(count):
        for k, which in spread_list[:count]:
            target = lax.rem(z - k + nz, nz)
            pltpu.make_async_remote_copy(
                src_ref=wt.at[which : which + 1, pl.ds(pl.multiple_of(target * hq, 16), hq), :],
                dst_ref=wall.at[sp, which : which + 1, 0:hq, :],
                send_sem=w_send.at[0],
                recv_sem=w_recv.at[w_index("z", k, which)],
                device_id=(2 * target + y, tp),
                device_id_type=MESH,
            ).start()
        del spread_list[:count]

    def hop_own(k, some=(0, 1, 2)):
        for which in some:
            weight_wait("z", k, thirds[which])
            for kind in ("y", "x", "cz"):
                weight_copy(kind, k, thirds[which]).start()

    def hop_side(k, some=(0, 1, 2)):
        for which in some:
            for kind, route in (("y", "x"), ("x", "y")):
                weight_wait(kind, k, thirds[which])
                if diagonal(k, which) == route:
                    weight_copy("d", k, thirds[which]).start()
                weight_copy("c" + kind, k, thirds[which]).start()

    def hop_far(k, some=(0, 1, 2)):
        for which in some:
            weight_wait("d", k, thirds[which])
            if k > 0:
                weight_copy("cd", k, thirds[which]).start()
        if k == 0:
            weight_copy("cd", k, whole[0]).start()

    send("k")
    locs["v"].wait()
    vbuf[sp] = vraw[...].T
    send("v")
    locs["g"].wait()
    locs["u"].wait()

    def transpose(i, carry):
        part = pl.ds(pl.multiple_of(i * 128, 128), 128)
        for which in range(2):
            wt[which, part, :] = raw[which, :, part].T
        return carry

    lax.fori_loop(0, hidden // 128, transpose, 0)
    locs["d"].wait()
    own_piece = pltpu.make_async_copy(
        wt.at[:, pl.ds(pl.multiple_of(z * hq, 16), hq), :], wall.at[sp, :, 0:hq, :], loc_sem.at[5]
    )
    own_piece.start()
    spread(2)
    own_piece.wait()
    weight_copy("x", 0, whole[0]).start()
    weight_copy("cz", 0, whole[0]).start()
    weight_copy("y", 0, thirds[0]).start()

    locs["q"].wait()
    for h in range(groups):
        qs[h] = turned(q_in[:, h * hd : (h + 1) * hd], qg_ref[...]).T
    m_s[...] = jnp.full_like(m_s, -1e30)
    l_s[...] = jnp.zeros_like(l_s)
    acc[...] = jnp.zeros_like(acc)
    factor = hd ** (-0.5) * math.log2(math.e)

    def attend(slots):
        def one(i, carry):
            slot = slots[0]
            if len(slots) > 1:
                slot = jnp.where(i == 0, slots[0], slots[1])
            for h in range(groups):
                scores = jnp.dot(kbuf[slot], qs[h], preferred_element_type=jnp.float32)
                before = m_s[h]
                highest = jnp.maximum(before, jnp.max(scores, axis=0, keepdims=True))
                scale = jnp.exp2((before - highest) * factor)
                probs = jnp.exp2((scores - highest) * factor)
                m_s[h] = highest
                l_s[h] = l_s[h] * scale + jnp.sum(probs, axis=0, keepdims=True)
                acc[h] = acc[h] * scale + jnp.dot(
                    vbuf[slot], probs.astype(jnp.bfloat16), preferred_element_type=jnp.float32
                )
            return carry

        lax.fori_loop(0, len(slots), one, 0)

    attend([sp])
    for step in range(1, half + 1):
        arrive("k", step)
        arrive("v", step)
        if step != half - 1:
            spread(1 if step < half else 3)
        if step < 3:
            weight_copy("y", 0, thirds[step]).start()
        if step == 2:
            hop_own(1, (0, 1))
        if step <= 3:
            weight_wait("y", 0, thirds[step - 1])
            weight_copy("d", 0, thirds[step - 1]).start()
        if step == half - 1:
            weight_copy("cy", 0, whole[0]).start()
            weight_wait("x", 0, whole[0])
            weight_copy("cx", 0, whole[0]).start()
            hop_own(1, (2,))
        ends = [ring_at(pos - step), ring_at(pos + step)]
        attend(ends if step < half else ends[:1])

    for h in range(groups):
        done = (acc[h] / l_s[h]).astype(jnp.bfloat16)
        for t in range(tn):
            att[t, :, h * hd : (h + 1) * hd] = done[:, t * rows : (t + 1) * rows].T
    for d in range(1, tn):
        peer = lax.rem(tp + d, tn)
        copy = pltpu.make_async_remote_copy(
            src_ref=att.at[peer],
            dst_ref=heads.at[tp],
            send_sem=tp_send.at[0],
            recv_sem=tp_recv.at[0],
            device_id=(sp, peer),
            device_id_type=MESH,
        )
        copy.start()
    heads[tp] = att[tp]
    hop_far(0)
    hop_side(1)
    hop_own(3, (0, 1))
    locs["o"].wait()
    locs["r"].wait()
    arrival(heads.at[0 : tn - 1], tp_recv.at[0]).wait_recv()

    span = math.gcd(ow.shape[1], 512)

    def project(i, carry):
        cols = pl.ds(pl.multiple_of(i * span, span), span)
        total = jnp.zeros((rows, span), jnp.float32)
        for t in range(tn):
            total += jnp.dot(
                heads[t], ow[t * width : (t + 1) * width, cols], preferred_element_type=jnp.float32
            )
        proj[:, cols] = total
        return carry

    lax.fori_loop(0, wide // span, project, 0)
    projected = proj[...]
    middle = (
        res_ref[...].astype(jnp.float32)
        + og_ref[...]
        * (projected * lax.rsqrt(jnp.mean(projected * projected, axis=-1, keepdims=True) + EPS))
    ).astype(jnp.bfloat16)
    mid[...] = middle
    middle = middle.astype(jnp.float32)
    normed = (
        mg_ref[...] * (middle * lax.rsqrt(jnp.mean(middle * middle, axis=-1, keepdims=True) + EPS))
    ).astype(jnp.bfloat16)

    ahead = {0: nz - 1 - z, 1: z}
    behind = {0: z, 1: nz - 1 - z}
    next_dev = {0: (lax.rem(sp + 2, n), tp), 1: (lax.rem(sp - 2 + n, n), tp)}
    side = rows // 2

    def line_rows(at):
        return pl.ds(pl.multiple_of(at * side, 16), side)

    def token_copy(part, way, e, lag):
        origin = z - (e - lag) if way == 0 else z + (e - lag)
        block = toks.at[part, line_rows(origin), :]
        index = (part * 2 + way) * (nz - 1) + e - 1
        return pltpu.make_async_remote_copy(
            src_ref=block,
            dst_ref=block,
            send_sem=t_send.at[index],
            recv_sem=t_recv.at[index],
            device_id=next_dev[way],
            device_id_type=MESH,
        )

    for part in range(2):
        toks[part, line_rows(z), :] = normed[part * side : (part + 1) * side]
    def token_send(part):
        for way in range(2):

            @pl.when(ahead[way] > 0)
            def _():
                token_copy(part, way, 1, 1).start()

    token_send(0)

    def token_hop(part, e):
        for way in range(2):

            @pl.when(jnp.logical_and(behind[way] >= e, ahead[way] > 0))
            def _():
                token_copy(part, way, e, 0).wait_recv()
                token_copy(part, way, e + 1, 1).start()

    def tokens_in(part):
        for way in range(2):

            @pl.when(ahead[way] == 0)
            def _():
                for e in range(1, nz):
                    token_copy(part, way, e, 0).wait_recv()

    def weights_in(late):
        arrival(wall.at[0 : 1 if late else nz - 1], w_recv.at[w_index("c", last if late else 0, 0)]).wait_recv()

    def feed(part, blocks, before=False, after=True):
        def feed_tile(r, carry):
            base = pl.multiple_of(r * hq, 16)
            branches = []
            for which in range(2):
                total = jnp.zeros((hq, nz * side), jnp.float32)
                for s in blocks:
                    total += lax.dot_general(
                        wall[s, which, pl.ds(base, hq), :],
                        toks[part, :, pl.ds(pl.multiple_of(s * depth, 128), depth)],
                        (((1,), (1,)), ((), ())),
                        preferred_element_type=jnp.float32,
                    )
                if before:
                    total += partial[which, pl.ds(base, hq), :]
                if after:
                    branches.append(total)
                else:
                    partial[which, pl.ds(base, hq), :] = total
            if after:
                gate, up = branches
                inner[pl.ds(base, hq), :] = (gate / (1.0 + jnp.exp(-gate)) * up).astype(jnp.bfloat16)
            return carry

        lax.fori_loop(0, tn, feed_tile, 0)

    early = [column(k, at) for k in range(nz) if k != last for at in range(2)]
    late = [column(last, at) for at in range(2)]

    cut = wide // 2
    halves = [slice(0, cut), slice(cut, wide)]
    full = [slice(0, wide)]

    def sum_copy(part, way, d, cols):
        index = (((part * 2 + way) * (nz - 1)) + d - 1) * 2 + cols.start // cut
        return pltpu.make_async_remote_copy(
            src_ref=psend.at[part, way, d - 1, :, cols],
            dst_ref=precv.at[part, way, d - 1, :, cols],
            send_sem=p_send.at[index],
            recv_sem=p_recv.at[index],
            device_id=next_dev[way],
            device_id_type=MESH,
        )

    def share(part, way, d, cols):
        owner = z + d if way == 0 else z - d
        return osc[part, line_rows(owner), cols]

    def down(part):
        for s in range(n):
            osc[part, :, s * depth : (s + 1) * depth] = lax.dot_general(
                inner[...],
                wall[s, 2],
                (((0,), (0,)), ((), ())),
                preferred_element_type=jnp.float32,
            )
        for way in range(2):

            @pl.when(behind[way] == 0)
            def _():
                for d in range(nz - 1, 0, -1):
                    for cols in halves if d == nz - 1 else full:
                        psend[part, way, d - 1, :, cols] = share(part, way, d, cols).astype(
                            jnp.bfloat16
                        )
                        sum_copy(part, way, d, cols).start()

    def pass_sums(part, way, d, pieces):
        for cols in pieces:
            sum_copy(part, way, d + 1, cols).wait_recv()
            psend[part, way, d - 1, :, cols] = (
                share(part, way, d, cols) + precv[part, way, d, :, cols].astype(jnp.float32)
            ).astype(jnp.bfloat16)
            sum_copy(part, way, d, cols).start()

    def collect(part):
        mine = slice(part * side, (part + 1) * side)
        for d in range(nz - 2, 0, -1):
            for way in range(2):

                @pl.when(jnp.logical_and(behind[way] > 0, ahead[way] == d))
                def _():
                    pass_sums(part, way, d, halves)

        for d in range(nz - 2, 0, -1):
            for way in range(2):

                @pl.when(jnp.logical_and(behind[way] > 0, ahead[way] > d))
                def _():
                    pass_sums(part, way, d, full)

        proj[mine] = share(part, 0, 0, full[0])
        for way in range(2):
            for pieces in (halves, full):

                @pl.when(jnp.logical_and(behind[way] > 0, ahead[way] == 0 if pieces is halves else ahead[way] > 0))
                def _():
                    for cols in pieces:
                        sum_copy(part, way, 1, cols).wait_recv()
                        proj[mine, cols] += precv[part, way, 0, :, cols].astype(jnp.float32)

        total = proj[mine]
        out_ref[mine] = (
            mid[mine].astype(jnp.float32)
            + fg_ref[...] * (total * lax.rsqrt(jnp.mean(total * total, axis=-1, keepdims=True) + EPS))
        ).astype(jnp.bfloat16)
        result(part).start()

    def result(part):
        mine = pl.ds(part * side, side)
        return pltpu.make_async_copy(out_ref.at[mine], out_hbm.at[mine], loc_sem.at[6 + part])

    spread(2)
    hop_own(3, (2,))
    hop_far(1)
    token_hop(0, 1)
    hop_side(3, (0,))
    hop_own(2, (0,))
    hop_side(3, (1, 2))
    hop_own(2, (1, 2))
    token_hop(0, 2)
    hop_side(2, (0,))
    token_send(1)
    hop_side(2, (1, 2))
    hop_far(3)
    weights_in(False)
    tokens_in(0)
    feed(0, early, after=False)
    token_hop(1, 1)
    hop_far(2)
    token_hop(1, 2)
    weights_in(True)
    feed(0, late, before=True)
    down(0)
    tokens_in(1)
    feed(1, range(n))
    down(1)
    collect(0)
    collect(1)
    arrival(kbuf.at[0 : n - 1], send_sem.at[0]).wait_send()
    arrival(vbuf.at[0 : n - 1], send_sem.at[1]).wait_send()
    arrival(att.at[0 : tn - 1], tp_send.at[0]).wait_send()
    arrival(wall.at[0, :, 0 : (nz - 1) * hq, :], w_send.at[0]).wait_send()
    arrival(wall.at[0 : nz - 1], w_send.at[1]).wait_send()
    arrival(wall.at[0:nz], w_send.at[2]).wait_send()

    for part in range(2):
        for way in range(2):
            for e in range(1, nz):

                @pl.when(jnp.logical_and(ahead[way] > 0, behind[way] >= e - 1))
                def _():
                    token_copy(part, way, e, 1).wait_send()

                for pieces in (halves, full):

                    @pl.when(ahead[way] == e if pieces is halves else ahead[way] > e)
                    def _():
                        for cols in pieces:
                            sum_copy(part, way, e, cols).wait_send()

    for part in range(2):
        result(part).wait()


def fused(n, tn, *args):
    (queries, keys, values, q_gain, k_gain, out_weight, out_gain, residual_in) = args[:8]
    (mlp_gain, gate_weight, up_weight, down_weight, final_gain) = args[8:]
    tok, hd = keys.shape
    groups = queries.shape[1] // hd
    depth, hidden = gate_weight.shape
    rows, wide = residual_in.shape
    vmem = pl.BlockSpec(memory_space=pltpu.VMEM)
    hbm = pl.BlockSpec(memory_space=pl.ANY)
    half = n // 2
    b16, f32 = jnp.bfloat16, jnp.float32
    return pl.pallas_call(
        functools.partial(layer_kernel, n, tn),
        out_shape=jax.ShapeDtypeStruct((rows, wide), b16),
        in_specs=[hbm, vmem, hbm, vmem, vmem, hbm, vmem, hbm, vmem, hbm, hbm, hbm, vmem],
        out_specs=hbm,
        scratch_shapes=[
            pltpu.VMEM((rows, wide), b16),
            pltpu.VMEM((tok, groups * hd), b16),
            pltpu.VMEM((rows, wide), b16),
            pltpu.VMEM((tok, hd), f32),
            pltpu.VMEM((tok, hd), f32),
            pltpu.VMEM((groups, hd, tok), b16),
            pltpu.VMEM((n, tok, hd), b16),
            pltpu.VMEM((n, hd, tok), b16),
            pltpu.VMEM((tok, hd), b16),
            pltpu.VMEM((2, depth, hidden), b16),
            pltpu.VMEM((3, hidden, depth), b16),
            pltpu.VMEM((n, 3, hidden // half * tn, depth), b16),
            pltpu.VMEM((wide, wide), b16),
            pltpu.VMEM((groups, 1, tok), f32),
            pltpu.VMEM((groups, 1, tok), f32),
            pltpu.VMEM((groups, hd, tok), f32),
            pltpu.VMEM((tn, rows, groups * hd), b16),
            pltpu.VMEM((tn, rows, groups * hd), b16),
            pltpu.VMEM((rows, wide), f32),
            pltpu.VMEM((rows, wide), b16),
            pltpu.VMEM((2, half * rows // 2, wide), b16),
            pltpu.VMEM((hidden // half * tn, half * rows // 2), b16),
            pltpu.VMEM((2, hidden // half * tn, half * rows // 2), f32),
            pltpu.VMEM((2, half * rows // 2, wide), f32),
            pltpu.VMEM((2, 2, half - 1, rows // 2, wide), b16),
            pltpu.VMEM((2, 2, half - 1, rows // 2, wide), b16),
            pltpu.SemaphoreType.DMA((10,)),
            pltpu.SemaphoreType.DMA((2,)),
            pltpu.SemaphoreType.DMA((4 * half,)),
            pltpu.SemaphoreType.DMA((1,)),
            pltpu.SemaphoreType.DMA((1,)),
            pltpu.SemaphoreType.DMA((3,)),
            pltpu.SemaphoreType.DMA((4 * half * 3 + 2,)),
            pltpu.SemaphoreType.DMA((4 * (half - 1),)),
            pltpu.SemaphoreType.DMA((4 * (half - 1),)),
            pltpu.SemaphoreType.DMA((8 * (half - 1),)),
            pltpu.SemaphoreType.DMA((8 * (half - 1),)),
        ],
        compiler_params=pltpu.CompilerParams(
            collective_id=0, has_side_effects=True, vmem_limit_bytes=67043328
        ),
    )(
        queries,
        keys,
        values,
        q_gain[None],
        k_gain[None],
        out_weight,
        out_gain[None],
        residual_in,
        mlp_gain[None],
        gate_weight,
        up_weight,
        down_weight,
        final_gain[None],
    )


def body(mesh, *args):
    n, tn = mesh.shape["sp"], mesh.shape["tp"]
    tok, hd = args[1].shape
    depth, hidden = args[9].shape
    fits = n % 2 == 0 and n == 8 and depth % 128 == 0 and hidden % 128 == 0
    fits = fits and tn == 4 and hidden % (8 * n) == 0 and args[7].shape[0] % 128 == 0
    if fits and tok % 256 == 0 and hd == 128:
        return fused(n, tn, *args)
    return on_device(*args)


def solution(mesh):
    return jax.shard_map(
        functools.partial(body, mesh),
        mesh=mesh,
        in_specs=(
            P("sp", "tp"),
            P("sp", "tp"),
            P("sp", "tp"),
            P(),
            P(),
            P(),
            P(),
            P(("sp", "tp"), None),
            P(),
            P("sp", "tp"),
            P("sp", "tp"),
            P("tp", "sp"),
            P(),
        ),
        out_specs=P(("sp", "tp"), None),
        check_vma=False,
    )
```
